128 devices in a mesh: sp: 32 (over z, y, core), tp: 4 (over x).
Axes of the slice: x: 4, y: 4, z: 4, core: 2. Of those that a mesh axis runs over, the one named last changes fastest.
Arguments:
- queries: bfloat16 [12288, 1024], P('sp', 'tp'), may hold values from -10 to 10
- key_rows: bfloat16 [12288, 256], P('sp', 'tp'), may hold values from -10 to 10
- value_rows: bfloat16 [12288, 256], P('sp', 'tp'), may hold values from -6 to 6
- key_logit: bfloat16 [12288, 4], P('sp', 'tp'), may hold values from -3 to 17
- head_offset: float32 [16], P('tp'), may hold values from -17.5 to -4
- stream: bfloat16 [12288, 2048], P(('sp', 'tp')), may hold values from -3 to 3
- out_weight: bfloat16 [1024, 2048], replicated, may hold values from -0.1875 to 0.1875
- norm_gain: float32 [2048], replicated, may hold values from 0.1 to 1.9
- expert_ids: int32 [12288, 2], P(('sp', 'tp')), may hold values from 0 to 127, as said below
- group_logit: float32 [12288], P(('sp', 'tp')), may hold values from -6 to 6
- expert_logits: float32 [12288, 2], P(('sp', 'tp')), may hold values from -6 to 6
- gate_weight: bfloat16 [128, 2048, 1024], P(('sp', 'tp')), may hold values from -0.125 to 0.125
- up_weight: bfloat16 [128, 2048, 1024], P(('sp', 'tp')), may hold values from -0.125 to 0.125
- down_weight: bfloat16 [128, 1024, 2048], P(('sp', 'tp')), may hold values from -0.1875 to 0.1875
Outputs:
- result: bfloat16 [12288, 2048], P(('sp', 'tp'))
The draws below stay inside these ranges and needn't reach their ends.
Inputs may be any that keep to these rules, and one draw needn't show every extreme that they name: `expert_ids`: the two numbers of a row differ and lie in one group of 4 consecutive numbers. In the rows of one device (aligned blocks of 96 rows) no number is named more than 3 times, and in every block some number is named exactly 3 times.
All inputs are finite; a program needn't handle non-finite values.
Results may differ from the reference program's by a relative error of at most 0.012.
Values may be sent and summed in bfloat16 or wider, within the bound.
A program may use at most 128 MiB of HBM per device.

```python
import math
import jax
import jax.numpy as jnp
from jax import lax

D = 2048
HEADS = 16
KV_HEADS = 4
HEAD_DIM = 64
FF = 1024
GROUP_EXPERTS = 4
TOP = 2
TOK_DEV = 384
TOKENS = 12288
ROWS_DEV = 96
EXPERTS = 128
GROUPS = 32
CAP = 3
N_SP = 32
N_TP = 4


def draw_head_offset(key, part):
    base_key = jax.random.fold_in(key, 11)
    pick_key, rate_key = jax.random.split(base_key)
    scores = jax.random.randint(pick_key, (HEADS,), 0, 4096) * HEADS + jnp.arange(HEADS)
    ranking = jnp.argsort(jnp.argsort(scores))
    slow_heads = ranking < HEADS // 2
    spread = jax.random.uniform(rate_key, (HEADS,), jnp.float32, 0.0, 1.5)
    slow_value = -(math.log(TOKENS) + 4.5 + spread)
    fast_value = -(4.5 + spread)
    return jnp.where(slow_heads, slow_value, fast_value).astype(jnp.float32)


def draw_key_logit(key, part):
    base_key = jax.random.fold_in(key, 23)
    level_key, noise_key, spot_key = jax.random.split(base_key, 3)
    block_count = TOKENS // TOK_DEV
    levels = jax.random.uniform(level_key, (block_count, 1, KV_HEADS), jnp.float32, -0.7, 0.7)
    noise = jnp.clip(0.5 * jax.random.normal(noise_key, (block_count, TOK_DEV, KV_HEADS), jnp.float32), -1.5, 1.5)
    base_value = (levels + noise).reshape(TOKENS, KV_HEADS)
    spots = jax.random.randint(spot_key, (3, KV_HEADS), 0, TOKENS)
    hits = jnp.sum((jnp.arange(TOKENS)[:, None, None] == spots[None, :, :]).astype(jnp.float32), axis=1)
    hits = jnp.minimum(hits, 1.0)
    return (base_value + hits * (math.log(TOKENS) + 4.0)).astype(jnp.bfloat16)


def draw_expert_ids(key, part):
    base_key = jax.random.fold_in(key, 37)
    hot_key, size_key, sign_key, order_key, label_key = jax.random.split(base_key, 5)
    block_count = TOKENS // ROWS_DEV
    pair_count = GROUPS // 2
    hot_expert = jax.random.randint(hot_key, (), 0, EXPERTS)
    hot_group = hot_expert // GROUP_EXPERTS
    hot_local = hot_expert % GROUP_EXPERTS
    moved = jax.random.randint(size_key, (block_count, pair_count), 0, CAP + 1)
    coin = 1 - 2 * jax.random.randint(sign_key, (block_count, pair_count), 0, 2)
    pair_index = jnp.arange(pair_count)
    forced = 1 - 2 * (hot_group % 2)
    signed = jnp.where(pair_index[None, :] == hot_group // 2, forced, coin) * moved
    group_rows = jnp.stack([CAP + signed, CAP - signed], axis=2).reshape(block_count, GROUPS)
    ends = jnp.cumsum(group_rows, axis=1)
    starts = ends - group_rows
    order_bits = jax.random.randint(order_key, (block_count, ROWS_DEV), 0, 65536) * ROWS_DEV + jnp.arange(ROWS_DEV)[None, :]
    position = jnp.argsort(order_bits, axis=1)
    row_group = jnp.sum((position[:, :, None] >= ends[:, None, :]).astype(jnp.int32), axis=2)
    local_index = position - jnp.take_along_axis(starts, row_group, axis=1)
    half_index = local_index // CAP
    label_bits = jax.random.randint(label_key, (block_count, GROUPS, GROUP_EXPERTS), 0, 65536) * GROUP_EXPERTS + jnp.arange(GROUP_EXPERTS)
    labels = jnp.argsort(label_bits, axis=2)
    shifted = (labels + hot_local - labels[:, :, 0:1]) % GROUP_EXPERTS
    labels = jnp.where((jnp.arange(GROUPS) == hot_group)[None, :, None], shifted, labels)
    row_labels = jnp.take_along_axis(labels, row_group[:, :, None], axis=1)
    first_local = jnp.take_along_axis(row_labels, half_index[:, :, None], axis=2)[:, :, 0]
    second_local = jnp.take_along_axis(row_labels, (half_index + 2)[:, :, None], axis=2)[:, :, 0]
    first_ids = row_group * GROUP_EXPERTS + first_local
    second_ids = row_group * GROUP_EXPERTS + second_local
    return jnp.stack([first_ids, second_ids], axis=2).reshape(TOKENS, TOP).astype(jnp.int32)


def shard_levels(key, extent, cuts, least, largest):
    level = 1.0
    for axis_at, shards_of in cuts:
        steps = jax.random.uniform(jax.random.fold_in(jax.random.fold_in(key, 6), axis_at), (shards_of,), jnp.float32, least / len(cuts), largest / len(cuts))
        level = level * jnp.repeat(jnp.exp(steps), extent[axis_at] // shards_of).reshape((-1,) + (1,) * (len(extent) - 1 - axis_at))
    return level


def bell_draw(key, shape, scale, bound, shards=(), kind=jnp.bfloat16):
    entries = jax.random.normal(key, shape, jnp.float32) * scale
    if len(shards) > 0:
        entries = shard_levels(key, shape, shards, -0.22, 0.18) * entries
    return jnp.clip(entries, min=-bound, max=bound).astype(kind)


def setup_inputs(seed: int = 0) -> dict:
    streams_of = jax.random.split(jax.random.key(seed), 15)
    queries = bell_draw(streams_of[0], (TOKENS, HEADS * HEAD_DIM), 1.75, 10.0, ((0, 32), (1, 4)))
    key_rows = bell_draw(streams_of[1], (TOKENS, KV_HEADS * HEAD_DIM), 1.75, 10.0, ((0, 32), (1, 4)))
    value_rows = bell_draw(streams_of[2], (TOKENS, KV_HEADS * HEAD_DIM), 1.0, 6.0, ((0, 32), (1, 4)))
    key_logit = draw_key_logit(jax.random.fold_in(streams_of[14], 71), 0)
    head_offset = draw_head_offset(jax.random.fold_in(streams_of[14], 71), 0)
    stream = bell_draw(streams_of[5], (TOKENS, D), 0.5, 3.0, ((0, 128),))
    out_weight = bell_draw(streams_of[6], (HEADS * HEAD_DIM, D), (HEADS * HEAD_DIM) ** -0.5, 0.1875)
    norm_gain = jnp.clip(1.0 + 0.18 * jax.random.normal(streams_of[7], (D,), jnp.float32), 0.1, 1.9)
    expert_ids = draw_expert_ids(jax.random.fold_in(streams_of[14], 71), 0)
    group_logit = bell_draw(streams_of[9], (TOKENS,), 1.5, 6.0, ((0, 128),), jnp.float32)
    expert_logits = bell_draw(streams_of[10], (TOKENS, TOP), 1.5, 6.0, ((0, 128),), jnp.float32)
    gate_weight = bell_draw(streams_of[11], (EXPERTS, D, FF), D ** -0.5, 0.125, ((0, 128),))
    up_weight = bell_draw(streams_of[12], (EXPERTS, D, FF), D ** -0.5, 0.125, ((0, 128),))
    down_weight = bell_draw(streams_of[13], (EXPERTS, FF, D), FF ** -0.5, 0.1875, ((0, 128),))
    return dict(queries=queries, key_rows=key_rows, value_rows=value_rows, key_logit=key_logit, head_offset=head_offset, stream=stream, out_weight=out_weight, norm_gain=norm_gain, expert_ids=expert_ids, group_logit=group_logit, expert_logits=expert_logits, gate_weight=gate_weight, up_weight=up_weight, down_weight=down_weight)


norm_eps = 1e-06

def head_attention(head_index, queries_t, keys_t, values_t, logits_t, head_offset):
    group_share = HEADS // KV_HEADS
    key_head = (head_index // group_share).astype(jnp.int32)
    query_head = queries_t[head_index]
    key_head_rows = keys_t[key_head]
    value_head_rows = values_t[key_head]
    key_bias = logits_t[key_head].astype(jnp.float32)
    offset = head_offset[head_index]
    block_count = TOKENS // TOK_DEV
    query_blocks = query_head.reshape(block_count, TOK_DEV, HEAD_DIM)
    key_positions = jnp.arange(TOKENS, dtype=jnp.int32)

    def one_block(inputs):
        block_rows, block_index = inputs
        scores = jnp.dot(block_rows, key_head_rows.T, preferred_element_type=jnp.float32) * HEAD_DIM ** (-0.5)
        scores = scores + offset + key_bias[None, :]
        query_positions = block_index * TOK_DEV + jnp.arange(TOK_DEV, dtype=jnp.int32)
        causal = key_positions[None, :] < query_positions[:, None]
        stay_log = jax.nn.log_sigmoid(-scores)
        keep_log = jnp.where(causal, stay_log, 0.0)
        later_log = jnp.concatenate([keep_log[:, 1:], jnp.zeros((TOK_DEV, 1), jnp.float32)], axis=1)
        survive = lax.cumsum(later_log, axis=1, reverse=True)
        weight = jnp.where(causal, jnp.exp(scores + stay_log + survive), 0.0).astype(jnp.bfloat16)
        return jnp.dot(weight, value_head_rows, preferred_element_type=jnp.float32).astype(jnp.bfloat16)
    blocks_out = lax.map(one_block, (query_blocks, jnp.arange(block_count, dtype=jnp.int32)))
    return blocks_out.reshape(TOKENS, HEAD_DIM)

def reference(queries, key_rows, value_rows, key_logit, head_offset, stream, out_weight, norm_gain, expert_ids, group_logit, expert_logits, gate_weight, up_weight, down_weight):
    queries_t = queries.reshape(TOKENS, HEADS, HEAD_DIM).transpose(1, 0, 2)
    keys_t = key_rows.reshape(TOKENS, KV_HEADS, HEAD_DIM).transpose(1, 0, 2)
    values_t = value_rows.reshape(TOKENS, KV_HEADS, HEAD_DIM).transpose(1, 0, 2)
    logits_t = key_logit.T

    def per_head(head_index):
        return head_attention(head_index, queries_t, keys_t, values_t, logits_t, head_offset)
    attended = lax.map(per_head, jnp.arange(HEADS, dtype=jnp.int32))
    attended = attended.transpose(1, 0, 2).reshape(TOKENS, HEADS * HEAD_DIM)
    mixed_rows = (stream.astype(jnp.float32) + jnp.dot(attended, out_weight, preferred_element_type=jnp.float32)).astype(jnp.bfloat16)
    mixed_wide = mixed_rows.astype(jnp.float32)
    normed = (mixed_wide * lax.rsqrt(lax.optimization_barrier(jnp.mean(mixed_wide * mixed_wide, axis=-1, keepdims=True)) + norm_eps) * norm_gain).astype(jnp.bfloat16)
    expert_exp = jnp.exp(expert_logits)
    route_weight = jax.nn.sigmoid(group_logit)[:, None] * expert_exp / lax.optimization_barrier(jnp.sum(expert_exp, axis=1, keepdims=True))
    flat_ids = expert_ids.reshape(-1)
    slot_order = jnp.argsort(flat_ids, stable=True).astype(jnp.int32)
    sorted_ids = flat_ids[slot_order]
    starts = jnp.searchsorted(sorted_ids, jnp.arange(EXPERTS, dtype=jnp.int32)).astype(jnp.int32)
    most_rows = N_SP * N_TP * CAP
    sorted_rows = jnp.concatenate([normed[slot_order // 2], jnp.zeros((most_rows, D), jnp.bfloat16)], axis=0)

    def one_expert(outputs, inputs):
        gate_one, up_one, down_one, start_row = inputs
        block_rows = lax.dynamic_slice_in_dim(sorted_rows, start_row, most_rows, 0)
        gate_act = jnp.dot(block_rows, gate_one, preferred_element_type=jnp.float32)
        upward = jnp.dot(block_rows, up_one, preferred_element_type=jnp.float32)
        hidden = (jax.nn.silu(gate_act) * upward).astype(jnp.bfloat16)
        produced = jnp.dot(hidden, down_one, preferred_element_type=jnp.float32).astype(jnp.bfloat16)
        return (lax.dynamic_update_slice_in_dim(outputs, produced, start_row, 0), None)
    outputs, ignored = lax.scan(one_expert, jnp.zeros((2 * TOKENS + most_rows, D), jnp.bfloat16), (gate_weight, up_weight, down_weight, starts))
    inverse = jnp.argsort(slot_order).astype(jnp.int32)
    expert_out = outputs[:2 * TOKENS][inverse].reshape(TOKENS, TOP, D).astype(jnp.float32)
    combined = mixed_wide + lax.optimization_barrier(jnp.sum(route_weight[:, :, None] * expert_out, axis=1))
    return combined.astype(jnp.bfloat16)
```

```python
import functools
import jax
import jax.numpy as jnp
from jax import lax
from jax.experimental import pallas as pl
from jax.experimental.pallas import tpu as pltpu
from jax.sharding import PartitionSpec as P

HEAD_DIM = 64
GROUP_EXPERTS = 4
TOP = 2


norm_eps = 1e-06


HEADS = 4
BLK = 384
HALF = 192
SEG = 48
CHUNK = 16
COLS = 768
TILE = 256
LOG2E = 1.4426950408889634


def split3(x):
    hi = x.astype(jnp.bfloat16).astype(jnp.float32)
    rest = x - hi
    mid = rest.astype(jnp.bfloat16).astype(jnp.float32)
    lo = (rest - mid).astype(jnp.bfloat16).astype(jnp.float32)
    return hi, mid, lo


def attention_kernel(n, pos_ref, kv_ref, q_ref, off_ref, out_ref, qt, lk, vt, acc, carry, okay, wts):
    i = pos_ref[0]
    f32, bf16 = jnp.float32, jnp.bfloat16
    for s in range(2):
        qs = q_ref[s * HALF:(s + 1) * HALF, :].astype(f32) * (LOG2E * HEAD_DIM ** -0.5)
        rows = jnp.concatenate([qs[:, h * 64:(h + 1) * 64] for h in range(HEADS)], axis=0)
        high = rows.astype(bf16).astype(f32)
        low = rows - high
        zero = jnp.zeros_like(rows)
        top = jnp.concatenate([high, zero], axis=1).T
        bottom = jnp.concatenate([zero, low], axis=1).T
        lane = lax.broadcasted_iota(jnp.int32, (8, COLS), 1)
        off = jnp.zeros((8, COLS), f32)
        for h in range(HEADS):
            inside = jnp.logical_and(lane >= h * HALF, lane < (h + 1) * HALF)
            off = jnp.where(inside, off_ref[h] * LOG2E, off)
        hi, mid, lo = split3(off)
        row = lax.broadcasted_iota(jnp.int32, (8, COLS), 0)
        c_hi = 1.4453125
        extra = jnp.where(row == 0, c_hi, jnp.where(row == 1, LOG2E - c_hi, jnp.where(row == 2, hi, jnp.where(row == 3, mid, jnp.where(row == 4, lo, 0.0)))))
        bottom = jnp.concatenate([extra, bottom[8:, :]], axis=0)
        qt[0:128, s * COLS:(s + 1) * COLS] = top.astype(bf16)
        qt[128:256, s * COLS:(s + 1) * COLS] = bottom.astype(bf16)

    sub = lax.broadcasted_iota(jnp.int32, (8, TILE), 0)

    def exclusive(p):
        e = jnp.where(sub == 7, 1.0, pltpu.roll(p, 7, 0))
        e = e * jnp.where(sub == 7, 1.0, pltpu.roll(e, 7, 0))
        e = e * jnp.where(sub >= 6, 1.0, pltpu.roll(e, 6, 0))
        e = e * jnp.where(sub >= 4, 1.0, pltpu.roll(e, 4, 0))
        return e

    def tile(base, at, is_a, diag, slow):
        col = pl.multiple_of(base + at, 128)
        here = pl.ds(col, TILE)
        z = jnp.dot(lk[...], qt[:, here], preferred_element_type=f32)
        if diag:
            lane = lax.broadcasted_iota(jnp.int32, (8, TILE), 1)
            query = (lane + at) % HALF + jnp.where(is_a, 0, HALF)
            limit = query - sub * SEG
        start = carry[:, here]
        if slow:
            p = jnp.ones((8, TILE), f32)
            for r in reversed(range(SEG)):
                beta = 1.0 / (1.0 + jnp.exp2(-z[r * 8:(r + 1) * 8, :]))
                if diag:
                    beta = jnp.where(r < limit, beta, 0.0)
                w = p * beta
                p = p - w
                wts[r * 8:(r + 1) * 8, :] = w
            e = exclusive(p)
            total = e[0:1, :] * p[0:1, :]
            e = e * start
            scales = [e] * (SEG // CHUNK)
        else:
            ends, good = [], None
            for ch in range(SEG // CHUNK):
                f = jnp.ones((8, TILE), f32)
                for r in range(ch * CHUNK, (ch + 1) * CHUNK):
                    x = jnp.exp2(z[r * 8:(r + 1) * 8, :])
                    if diag:
                        x = jnp.where(r < limit, x, 0.0)
                    w = x * f
                    f = f + w
                    wts[r * 8:(r + 1) * 8, :] = w
                fine = jnp.where(f < 1e36, 1.0, 0.0)
                good = fine if good is None else jnp.minimum(good, fine)
                ends.append(1.0 / f)
            okay[:, 0:TILE] = jnp.minimum(okay[:, 0:TILE], good)
            p = ends[0] * ends[1] * ends[2]
            e = exclusive(p)
            total = e[0:1, :] * p[0:1, :]
            e = e * start
            s2 = e * ends[2]
            s1 = s2 * ends[1]
            scales = [s1 * ends[0], s1, s2]
        carry[:, here] = start * total
        both = [jnp.concatenate([s, s], axis=0) for s in scales]
        parts = []
        for r in range(0, SEG, 2):
            parts.append((wts[r * 8:(r + 2) * 8, :] * both[r // CHUNK]).astype(bf16))
        weight = jnp.concatenate(parts, axis=0)
        acc[:, here] += jnp.dot(vt[...], weight, preferred_element_type=f32)

    def sweep(slow):
        acc[...] = jnp.zeros_like(acc)
        carry[...] = jnp.ones_like(carry)

        def step(s, c):
            is_a = s <= i
            block = jnp.where(is_a, i - s, n - s)
            base = jnp.where(is_a, 0, COLS)
            rows = kv_ref[block, 0:BLK, :]
            lk[:, 0:128] = rows
            wide = rows.astype(f32)
            turned = pltpu.roll(wide, 64, 1)
            logit = kv_ref[block, BLK:BLK + 8, :].astype(f32)
            lane = lax.broadcasted_iota(jnp.int32, (128, 128), 1)
            for j in range(3):
                column = jnp.broadcast_to(logit[j:j + 1, :], (128, 128)).T
                side = jnp.where(lane < 2, column, jnp.where(lane < 5, 1.0, jnp.where(lane < 64, 0.0, turned[j * 128:(j + 1) * 128, :])))
                lk[j * 128:(j + 1) * 128, 128:256] = side.astype(bf16)
            vt[...] = wide.T[64:128, :].astype(bf16)
            edge = jnp.logical_or(s == 0, s == i + 1)

            @pl.when(edge)
            def _():
                for at in range(0, COLS, TILE):
                    tile(base, at, is_a, True, slow)

            @pl.when(jnp.logical_not(edge))
            def _():
                for at in range(0, COLS, TILE):
                    tile(base, at, is_a, False, slow)
            return c

        lax.fori_loop(0, n + 1, step, 0)

    okay[...] = jnp.ones_like(okay)
    sweep(False)

    @pl.when(jnp.min(okay[...]) < 0.5)
    def _():
        sweep(True)

    stacked = jnp.concatenate([acc[:, 0:COLS], acc[:, COLS:2 * COLS]], axis=0).T
    for s in range(2):
        heads = [stacked[h * HALF:(h + 1) * HALF, s * 64:(s + 1) * 64] for h in range(HEADS)]
        out_ref[s * HALF:(s + 1) * HALF, :] = jnp.concatenate(heads, axis=1).astype(bf16)


def attention(n, position, kv, q, offsets):
    vm = pl.BlockSpec(memory_space=pltpu.VMEM)
    sm = pl.BlockSpec(memory_space=pltpu.SMEM)
    return pl.pallas_call(
        functools.partial(attention_kernel, n),
        out_shape=jax.ShapeDtypeStruct((BLK, HEADS * HEAD_DIM), jnp.bfloat16),
        in_specs=[sm, vm, vm, sm],
        out_specs=vm,
        scratch_shapes=[
            pltpu.VMEM((256, 2 * COLS), jnp.bfloat16),
            pltpu.VMEM((BLK, 256), jnp.bfloat16),
            pltpu.VMEM((64, BLK), jnp.bfloat16),
            pltpu.VMEM((64, 2 * COLS), jnp.float32),
            pltpu.VMEM((8, 2 * COLS), jnp.float32),
            pltpu.VMEM((8, TILE), jnp.float32),
            pltpu.VMEM((BLK, TILE), jnp.float32),
        ],
        compiler_params=pltpu.CompilerParams(vmem_limit_bytes=40 * 1024 * 1024),
        name="attention",
    )(position, kv, q, offsets)


def pack_block(key_rows, value_rows, key_logit):
    both = jnp.concatenate([key_rows, value_rows], axis=1)
    both = both.reshape(8, SEG, 128).transpose(1, 0, 2).reshape(BLK, 128)
    logit = key_logit.reshape(8, SEG).T.reshape(3, 128)
    return jnp.concatenate([both, logit, jnp.zeros((13, 128), jnp.bfloat16)], axis=0)


def expert_apply(incoming, gate_one, up_one, down_one):
    flat_rows = incoming.reshape(-1, incoming.shape[-1])
    gate_act = jnp.dot(flat_rows, gate_one, preferred_element_type=jnp.float32)
    upward = jnp.dot(flat_rows, up_one, preferred_element_type=jnp.float32)
    hidden = (jax.nn.silu(gate_act) * upward).astype(jnp.bfloat16)
    produced = jnp.dot(hidden, down_one, preferred_element_type=jnp.float32).astype(jnp.bfloat16)
    return produced.reshape(incoming.shape)


def on_device(
    queries,
    key_rows,
    value_rows,
    key_logit,
    head_offset,
    stream,
    out_weight,
    norm_gain,
    expert_ids,
    group_logit,
    expert_logits,
    gate_weight,
    up_weight,
    down_weight,
):
    n = lax.axis_size("sp")
    position = lax.axis_index("sp").astype(jnp.int32).reshape(1)
    mirror = [(a, n - 1 - a) for a in range(n)]
    block = pack_block(key_rows, value_rows, key_logit)
    kv = lax.all_gather(block, "sp", axis=0)
    late = lax.ppermute(queries[HALF:], "sp", mirror)
    halves = attention(n, position, kv, jnp.concatenate([queries[:HALF], late], axis=0), head_offset)
    attended = jnp.concatenate([halves[:HALF], lax.ppermute(halves[HALF:], "sp", mirror)], axis=0)
    token_heads = lax.all_to_all(attended, "tp", split_axis=0, concat_axis=1, tiled=True)
    mixed_rows = (
        stream.astype(jnp.float32)
        + jnp.dot(token_heads, out_weight, preferred_element_type=jnp.float32)
    ).astype(jnp.bfloat16)
    mixed_wide = mixed_rows.astype(jnp.float32)
    normed = (
        mixed_wide
        * lax.rsqrt(jnp.mean(mixed_wide * mixed_wide, axis=-1, keepdims=True) + norm_eps)
        * norm_gain
    ).astype(jnp.bfloat16)
    expert_exp = jnp.exp(expert_logits)
    route_weight = (
        jax.nn.sigmoid(group_logit)[:, None]
        * expert_exp
        / jnp.sum(expert_exp, axis=1, keepdims=True)
    )
    rows_count = stream.shape[0]
    expert_total = gate_weight.shape[0] * lax.axis_size("sp") * lax.axis_size("tp")
    capacity = rows_count * GROUP_EXPERTS // expert_total
    flat_ids = expert_ids.reshape(-1)
    matches = (flat_ids[:, None] == jnp.arange(expert_total, dtype=jnp.int32)[None, :]).astype(
        jnp.int32
    )
    ranking = jnp.sum(jnp.cumsum(matches, axis=0) * matches, axis=1) - 1
    slot_index = flat_ids * capacity + ranking
    chooser = jnp.arange(expert_total * capacity, dtype=jnp.int32)[:, None] == slot_index[None, :]
    chooser = jnp.sum(
        chooser.reshape(expert_total * capacity, rows_count, TOP).astype(jnp.int32), axis=2
    ).astype(jnp.bfloat16)
    outgoing = jnp.dot(chooser, normed, preferred_element_type=jnp.float32).astype(jnp.bfloat16)
    outgoing = outgoing.reshape(expert_total, capacity, -1)
    produced = expert_apply(
        lax.all_to_all(outgoing, ("sp", "tp"), split_axis=0, concat_axis=0, tiled=True),
        gate_weight[0],
        up_weight[0],
        down_weight[0],
    )
    returned = lax.all_to_all(produced, ("sp", "tp"), split_axis=0, concat_axis=0, tiled=True)
    back_rows = returned.reshape(expert_total * capacity, -1)
    picked = (
        jnp.take(back_rows, slot_index, axis=0).reshape(rows_count, TOP, -1).astype(jnp.float32)
    )
    combined = mixed_wide + jnp.sum(route_weight[:, :, None] * picked, axis=1)
    return combined.astype(jnp.bfloat16)


def solution(mesh):
    placed = (
        P("sp", "tp"),
        P("sp", "tp"),
        P("sp", "tp"),
        P("sp", "tp"),
        P("tp"),
        P(("sp", "tp"), None),
        P(),
        P(),
        P(("sp", "tp"), None),
        P(("sp", "tp")),
        P(("sp", "tp"), None),
        P(("sp", "tp"), None, None),
        P(("sp", "tp"), None, None),
        P(("sp", "tp"), None, None),
    )
    return jax.shard_map(
        on_device, mesh=mesh, in_specs=placed, out_specs=P(("sp", "tp"), None), check_vma=False
    )
```

```python
import functools

import jax
import jax.numpy as jnp
from jax import lax
from jax.experimental import pallas as pl
from jax.experimental.pallas import tpu as pltpu
from jax.sharding import PartitionSpec as P

HEAD_DIM = 64
GROUP_EXPERTS = 4
TOP = 2


norm_eps = 1e-06


HEADS = 4
BLK = 384
HALF = 192
SEG = 48
CHUNK = 16
COLS = 768
TILE = 256
LOG2E = 1.4426950408889634


def split3(x):
    hi = x.astype(jnp.bfloat16).astype(jnp.float32)
    rest = x - hi
    mid = rest.astype(jnp.bfloat16).astype(jnp.float32)
    lo = (rest - mid).astype(jnp.bfloat16).astype(jnp.float32)
    return hi, mid, lo


def attention_kernel(n, pos_ref, kv_ref, q_ref, off_ref, out_ref, qt, lk, vt, acc, carry, okay, wts):
    i = pos_ref[0]
    f32, bf16 = jnp.float32, jnp.bfloat16
    for s in range(2):
        qs = q_ref[s * HALF:(s + 1) * HALF, :].astype(f32) * (LOG2E * HEAD_DIM ** -0.5)
        rows = jnp.concatenate([qs[:, h * 64:(h + 1) * 64] for h in range(HEADS)], axis=0)
        high = rows.astype(bf16).astype(f32)
        low = rows - high
        zero = jnp.zeros_like(rows)
        top = jnp.concatenate([high, zero], axis=1).T
        bottom = jnp.concatenate([zero, low], axis=1).T
        lane = lax.broadcasted_iota(jnp.int32, (8, COLS), 1)
        off = jnp.zeros((8, COLS), f32)
        for h in range(HEADS):
            inside = jnp.logical_and(lane >= h * HALF, lane < (h + 1) * HALF)
            off = jnp.where(inside, off_ref[h] * LOG2E, off)
        hi, mid, lo = split3(off)
        row = lax.broadcasted_iota(jnp.int32, (8, COLS), 0)
        c_hi = 1.4453125
        extra = jnp.where(row == 0, c_hi, jnp.where(row == 1, LOG2E - c_hi, jnp.where(row == 2, hi, jnp.where(row == 3, mid, jnp.where(row == 4, lo, 0.0)))))
        bottom = jnp.concatenate([extra, bottom[8:, :]], axis=0)
        qt[s, 0:128, :] = top.astype(bf16)
        qt[s, 128:256, :] = bottom.astype(bf16)

    sub = lax.broadcasted_iota(jnp.int32, (8, TILE), 0)

    def exclusive(p):
        e = jnp.where(sub == 7, 1.0, pltpu.roll(p, 7, 0))
        e = e * jnp.where(sub == 7, 1.0, pltpu.roll(e, 7, 0))
        e = e * jnp.where(sub >= 6, 1.0, pltpu.roll(e, 6, 0))
        e = e * jnp.where(sub >= 4, 1.0, pltpu.roll(e, 4, 0))
        return e

    def tile(half, at, is_a, diag, slow, start):
        here = slice(at, at + TILE)
        z = jnp.dot(lk[...], qt[half, :, here], preferred_element_type=f32)
        if diag:
            lane = lax.broadcasted_iota(jnp.int32, (8, TILE), 1)
            query = (lane + at) % HALF + jnp.where(is_a, 0, HALF)
            limit = query - sub * SEG
        if slow:
            p = jnp.ones((8, TILE), f32)
            for r in reversed(range(SEG)):
                beta = 1.0 / (1.0 + jnp.exp2(-z[r * 8:(r + 1) * 8, :]))
                if diag:
                    beta = jnp.where(r < limit, beta, 0.0)
                w = p * beta
                p = p - w
                wts[r * 8:(r + 1) * 8, here] = w
            e = exclusive(p)
            total = e[0:1, :] * p[0:1, :]
            e = e * start
            scales = [e] * (SEG // CHUNK)
        else:
            ends, good = [], None
            for ch in range(SEG // CHUNK):
                f = jnp.ones((8, TILE), f32)
                for r in range(ch * CHUNK, (ch + 1) * CHUNK):
                    x = jnp.exp2(z[r * 8:(r + 1) * 8, :])
                    if diag:
                        x = jnp.where(r < limit, x, 0.0)
                    w = x * f
                    f = f + w
                    wts[r * 8:(r + 1) * 8, here] = w
                fine = jnp.where(f < 1e36, 1.0, 0.0)
                good = fine if good is None else jnp.minimum(good, fine)
                ends.append(1.0 / f)
            okay[:, here] = jnp.minimum(okay[:, here], good)
            p = ends[0] * ends[1] * ends[2]
            e = exclusive(p)
            total = e[0:1, :] * p[0:1, :]
            e = e * start
            s2 = e * ends[2]
            s1 = s2 * ends[1]
            scales = [s1 * ends[0], s1, s2]
        both = [jnp.concatenate([s, s], axis=0) for s in scales]
        parts = []
        for r in range(0, SEG, 2):
            parts.append((wts[r * 8:(r + 2) * 8, here] * both[r // CHUNK]).astype(bf16))
        weight = jnp.concatenate(parts, axis=0)
        return start * total, jnp.dot(vt[...], weight, preferred_element_type=f32)

    def tiles(half, is_a, diag, slow):
        spots = range(0, COLS, TILE)
        starts = [carry[half, :, at:at + TILE] for at in spots]
        done = [tile(half, at, is_a, diag, slow, start) for at, start in zip(spots, starts)]
        for at, (left, added) in zip(spots, done):
            carry[half, :, at:at + TILE] = left
            acc[half, :, at:at + TILE] += added

    def sweep(slow):
        acc[...] = jnp.zeros_like(acc)
        carry[...] = jnp.ones_like(carry)

        def step(s, c):
            is_a = s <= i
            block = jnp.where(is_a, i - s, n - s)
            half = jnp.where(is_a, 0, 1)
            rows = kv_ref[block, 0:BLK, :]
            lk[:, 0:128] = rows
            wide = rows.astype(f32)
            turned = pltpu.roll(wide, 64, 1)
            logit = kv_ref[block, BLK:BLK + 8, :].astype(f32)
            lane = lax.broadcasted_iota(jnp.int32, (128, 128), 1)
            for j in range(3):
                column = jnp.broadcast_to(logit[j:j + 1, :], (128, 128)).T
                side = jnp.where(lane < 2, column, jnp.where(lane < 5, 1.0, jnp.where(lane < 64, 0.0, turned[j * 128:(j + 1) * 128, :])))
                lk[j * 128:(j + 1) * 128, 128:256] = side.astype(bf16)
            vt[...] = wide.T[64:128, :].astype(bf16)
            edge = jnp.logical_or(s == 0, s == i + 1)

            @pl.when(edge)
            def _():
                tiles(half, is_a, True, slow)

            @pl.when(jnp.logical_not(edge))
            def _():
                tiles(half, is_a, False, slow)
            return c

        lax.fori_loop(0, n + 1, step, 0)

    okay[...] = jnp.ones_like(okay)
    sweep(False)

    @pl.when(jnp.min(okay[...]) < 0.5)
    def _():
        sweep(True)

    stacked = jnp.concatenate([acc[0], acc[1]], axis=0).T
    for s in range(2):
        heads = [stacked[h * HALF:(h + 1) * HALF, s * 64:(s + 1) * 64] for h in range(HEADS)]
        out_ref[s * HALF:(s + 1) * HALF, :] = jnp.concatenate(heads, axis=1).astype(bf16)


def attention(n, position, kv, q, offsets):
    vm = pl.BlockSpec(memory_space=pltpu.VMEM)
    sm = pl.BlockSpec(memory_space=pltpu.SMEM)
    return pl.pallas_call(
        functools.partial(attention_kernel, n),
        out_shape=jax.ShapeDtypeStruct((BLK, HEADS * HEAD_DIM), jnp.bfloat16),
        in_specs=[sm, vm, vm, sm],
        out_specs=vm,
        scratch_shapes=[
            pltpu.VMEM((2, 256, COLS), jnp.bfloat16),
            pltpu.VMEM((BLK, 256), jnp.bfloat16),
            pltpu.VMEM((64, BLK), jnp.bfloat16),
            pltpu.VMEM((2, 64, COLS), jnp.float32),
            pltpu.VMEM((2, 8, COLS), jnp.float32),
            pltpu.VMEM((8, COLS), jnp.float32),
            pltpu.VMEM((BLK, COLS), jnp.float32),
        ],
        compiler_params=pltpu.CompilerParams(vmem_limit_bytes=40 * 1024 * 1024),
        name="attention",
    )(position, kv, q, offsets)


ROWS = 400
CUT = 192
MESH = pl.DeviceIdType.MESH


def gather_kernel(n, k_ref, v_ref, l_ref, q_ref, kv_ref, qs_ref, send, recv):
    f32, bf16 = jnp.float32, jnp.bfloat16
    me = lax.axis_index("sp")
    z, y, core = me // 8, (me // 2) % 4, me % 2

    def at(a, b, c):
        dz, dy = a * c + b * (1 - c), a * (1 - c) + b * c
        return ((z + dz + 4) % 4) * 8 + ((y + dy + 4) % 4) * 2 + c

    other, mirror = me + 1 - 2 * core, n - 1 - me
    near = [at(1, 0, core), at(3, 0, core)], [at(0, 1, core), at(0, 3, core)]
    barrier = pltpu.get_barrier_semaphore()
    for peer in near[0] + near[1] + [other, mirror]:
        pl.semaphore_signal(barrier, inc=1, device_id={"sp": peer}, device_id_type=MESH)

    spot = lax.broadcasted_iota(jnp.int32, (BLK, BLK), 0)
    source = lax.broadcasted_iota(jnp.int32, (BLK, BLK), 1)
    order = jnp.where(source == (spot % 8) * SEG + spot // 8, 1.0, 0.0).astype(bf16)
    both = jnp.concatenate([k_ref[...], v_ref[...]], axis=1)
    kv_ref[me, 0:BLK, :] = jnp.dot(order, both, preferred_element_type=f32).astype(bf16)
    logit = jnp.broadcast_to(l_ref[...].astype(f32), (BLK, 128)).astype(bf16)
    logit = jnp.dot(order, logit, preferred_element_type=f32)
    row = lax.broadcasted_iota(jnp.int32, (16, 128), 0)
    tail = jnp.zeros((16, 128), f32)
    for j in range(3):
        tail = jnp.where(row == j, logit[j * 128:(j + 1) * 128, :].T[0:16, :], tail)
    kv_ref[me, BLK:ROWS, :] = tail.astype(bf16)
    qs_ref[0:HALF, :] = q_ref[0:HALF, :]
    pl.semaphore_wait(barrier, 6)

    begun = []
    parts = (slice(0, ROWS), slice(0, CUT), slice(CUT, ROWS))

    def copy(index, slot, part, peer):
        piece = kv_ref.at[slot, parts[part]]
        return pltpu.make_async_remote_copy(
            src_ref=piece, dst_ref=piece, send_sem=send.at[index], recv_sem=recv.at[index],
            device_id={"sp": peer}, device_id_type=MESH)

    def begin(index, slot, part, peer):
        c = copy(index, slot, part, peer)
        c.start()
        begun.append(c)

    def arrive(index, slot, part):
        copy(index, slot, part, me).wait_recv()

    around = (0, 3, 1, 2)

    def spread(k, a):
        slot = at(a, 0, core)
        for d in range(2):
            begin(4 + 4 * k + d, slot, 0, near[1][d])
        begin(20 + k, slot, 0, other)

    swap = pltpu.make_async_remote_copy(
        src_ref=q_ref.at[HALF:BLK], dst_ref=qs_ref.at[HALF:BLK], send_sem=send.at[36], recv_sem=recv.at[36],
        device_id={"sp": mirror}, device_id_type=MESH)
    for d in range(2):
        begin(d, me, 0, near[0][d])
    spread(0, 0)
    swap.start()
    for d, a in ((0, 3), (1, 1)):
        slot = at(a, 0, core)
        arrive(d, slot, 0)
        begin(2 + d, slot, 1 + d, near[0][d])
        spread(1 + d, a)
    for k, a in enumerate(around):
        if k == 3:
            slot = at(2, 0, core)
            for d in range(2):
                arrive(2 + d, slot, 1 + d)
            spread(3, 2)
        for d, b in ((0, 3), (1, 1)):
            slot = at(a, b, core)
            arrive(4 + 4 * k + d, slot, 0)
            begin(6 + 4 * k + d, slot, 1 + d, near[1][d])
            begin(24 + 4 * d + k, slot, 0, other)
    for k, a in enumerate(around):
        slot = at(a, 2, core)
        for d in range(2):
            arrive(6 + 4 * k + d, slot, 1 + d)
        begin(32 + k, slot, 0, other)
    for j, b in enumerate((0, 3, 1, 2)):
        for k, a in enumerate(around):
            arrive(20 + 4 * j + k, at(a, b, 1 - core), 0)
    swap.wait_recv()
    for c in begun:
        c.wait_send()
    swap.wait_send()


def gather(n, k, v, logit, q):
    vm = pl.BlockSpec(memory_space=pltpu.VMEM)
    return pl.pallas_call(
        functools.partial(gather_kernel, n),
        out_shape=(
            jax.ShapeDtypeStruct((n, ROWS, 128), jnp.bfloat16),
            jax.ShapeDtypeStruct((BLK, HEADS * HEAD_DIM), jnp.bfloat16),
        ),
        in_specs=[vm] * 4,
        out_specs=(vm, vm),
        scratch_shapes=[pltpu.SemaphoreType.DMA((37,)), pltpu.SemaphoreType.DMA((37,))],
        compiler_params=pltpu.CompilerParams(collective_id=0, has_side_effects=True, vmem_limit_bytes=24 * 1024 * 1024),
        name="gather",
    )(k, v, logit, q)


def expert_apply(incoming, gate_one, up_one, down_one):
    flat_rows = incoming.reshape(-1, incoming.shape[-1])
    gate_act = jnp.dot(flat_rows, gate_one, preferred_element_type=jnp.float32)
    upward = jnp.dot(flat_rows, up_one, preferred_element_type=jnp.float32)
    hidden = (jax.nn.silu(gate_act) * upward).astype(jnp.bfloat16)
    produced = jnp.dot(hidden, down_one, preferred_element_type=jnp.float32).astype(jnp.bfloat16)
    return produced.reshape(incoming.shape)


def on_device(
    queries,
    key_rows,
    value_rows,
    key_logit,
    head_offset,
    stream,
    out_weight,
    norm_gain,
    expert_ids,
    group_logit,
    expert_logits,
    gate_weight,
    up_weight,
    down_weight,
):
    n = lax.axis_size("sp")
    position = lax.axis_index("sp").astype(jnp.int32).reshape(1)
    mirror = [(a, n - 1 - a) for a in range(n)]
    kv, chosen = gather(n, key_rows, value_rows, key_logit, queries)
    halves = attention(n, position, kv, chosen, head_offset)
    attended = jnp.concatenate([halves[:HALF], lax.ppermute(halves[HALF:], "sp", mirror)], axis=0)
    token_heads = lax.all_to_all(attended, "tp", split_axis=0, concat_axis=1, tiled=True)
    mixed_rows = (
        stream.astype(jnp.float32)
        + jnp.dot(token_heads, out_weight, preferred_element_type=jnp.float32)
    ).astype(jnp.bfloat16)
    mixed_wide = mixed_rows.astype(jnp.float32)
    normed = (
        mixed_wide
        * lax.rsqrt(jnp.mean(mixed_wide * mixed_wide, axis=-1, keepdims=True) + norm_eps)
        * norm_gain
    ).astype(jnp.bfloat16)
    expert_exp = jnp.exp(expert_logits)
    route_weight = (
        jax.nn.sigmoid(group_logit)[:, None]
        * expert_exp
        / jnp.sum(expert_exp, axis=1, keepdims=True)
    )
    rows_count = stream.shape[0]
    expert_total = gate_weight.shape[0] * lax.axis_size("sp") * lax.axis_size("tp")
    capacity = rows_count * GROUP_EXPERTS // expert_total
    flat_ids = expert_ids.reshape(-1)
    matches = (flat_ids[:, None] == jnp.arange(expert_total, dtype=jnp.int32)[None, :]).astype(
        jnp.int32
    )
    ranking = jnp.sum(jnp.cumsum(matches, axis=0) * matches, axis=1) - 1
    slot_index = flat_ids * capacity + ranking
    chooser = jnp.arange(expert_total * capacity, dtype=jnp.int32)[:, None] == slot_index[None, :]
    chooser = jnp.sum(
        chooser.reshape(expert_total * capacity, rows_count, TOP).astype(jnp.int32), axis=2
    ).astype(jnp.bfloat16)
    outgoing = jnp.dot(chooser, normed, preferred_element_type=jnp.float32).astype(jnp.bfloat16)
    outgoing = outgoing.reshape(expert_total, capacity, -1)
    produced = expert_apply(
        lax.all_to_all(outgoing, ("sp", "tp"), split_axis=0, concat_axis=0, tiled=True),
        gate_weight[0],
        up_weight[0],
        down_weight[0],
    )
    returned = lax.all_to_all(produced, ("sp", "tp"), split_axis=0, concat_axis=0, tiled=True)
    back_rows = returned.reshape(expert_total * capacity, -1)
    picked = (
        jnp.take(back_rows, slot_index, axis=0).reshape(rows_count, TOP, -1).astype(jnp.float32)
    )
    combined = mixed_wide + jnp.sum(route_weight[:, :, None] * picked, axis=1)
    return combined.astype(jnp.bfloat16)


def solution(mesh):
    placed = (
        P("sp", "tp"),
        P("sp", "tp"),
        P("sp", "tp"),
        P("sp", "tp"),
        P("tp"),
        P(("sp", "tp"), None),
        P(),
        P(),
        P(("sp", "tp"), None),
        P(("sp", "tp")),
        P(("sp", "tp"), None),
        P(("sp", "tp"), None, None),
        P(("sp", "tp"), None, None),
        P(("sp", "tp"), None, None),
    )
    return jax.shard_map(
        on_device, mesh=mesh, in_specs=placed, out_specs=P(("sp", "tp"), None), check_vma=False
    )
```

```python
import functools

import jax
import jax.numpy as jnp
from jax import lax
from jax.experimental import pallas as pl
from jax.experimental.pallas import tpu as pltpu
from jax.sharding import PartitionSpec as P

HEAD_DIM = 64
norm_eps = 1e-06
HEADS = 4
BLK = 384
HALF = 192
SEG = 48
CHUNK = 16
COLS = 768
TILE = 256
LOG2E = 1.4426950408889634


def split3(x):
    hi = x.astype(jnp.bfloat16).astype(jnp.float32)
    rest = x - hi
    mid = rest.astype(jnp.bfloat16).astype(jnp.float32)
    lo = (rest - mid).astype(jnp.bfloat16).astype(jnp.float32)
    return hi, mid, lo


def attention_kernel(n, pos_ref, kv_ref, q_ref, off_ref, out_ref, qt, lk, vt, acc, carry, okay, wts):
    i = pos_ref[0]
    f32, bf16 = jnp.float32, jnp.bfloat16
    for s in range(2):
        qs = q_ref[s * HALF:(s + 1) * HALF, :].astype(f32) * (LOG2E * HEAD_DIM ** -0.5)
        rows = jnp.concatenate([qs[:, h * 64:(h + 1) * 64] for h in range(HEADS)], axis=0)
        high = rows.astype(bf16).astype(f32)
        low = rows - high
        zero = jnp.zeros_like(rows)
        top = jnp.concatenate([high, zero], axis=1).T
        bottom = jnp.concatenate([zero, low], axis=1).T
        lane = lax.broadcasted_iota(jnp.int32, (8, COLS), 1)
        off = jnp.zeros((8, COLS), f32)
        for h in range(HEADS):
            inside = jnp.logical_and(lane >= h * HALF, lane < (h + 1) * HALF)
            off = jnp.where(inside, off_ref[h] * LOG2E, off)
        hi, mid, lo = split3(off)
        row = lax.broadcasted_iota(jnp.int32, (8, COLS), 0)
        c_hi = 1.4453125
        extra = jnp.where(row == 0, c_hi, jnp.where(row == 1, LOG2E - c_hi, jnp.where(row == 2, hi, jnp.where(row == 3, mid, jnp.where(row == 4, lo, 0.0)))))
        bottom = jnp.concatenate([extra, bottom[8:, :]], axis=0)
        qt[s, 0:128, :] = top.astype(bf16)
        qt[s, 128:256, :] = bottom.astype(bf16)

    sub = lax.broadcasted_iota(jnp.int32, (8, TILE), 0)

    def exclusive(p):
        e = jnp.where(sub == 7, 1.0, pltpu.roll(p, 7, 0))
        e = e * jnp.where(sub == 7, 1.0, pltpu.roll(e, 7, 0))
        e = e * jnp.where(sub >= 6, 1.0, pltpu.roll(e, 6, 0))
        e = e * jnp.where(sub >= 4, 1.0, pltpu.roll(e, 4, 0))
        return e

    def tile(half, at, is_a, diag, slow, start):
        here = slice(at, at + TILE)
        z = jnp.dot(lk[...], qt[half, :, here], preferred_element_type=f32)
        if diag:
            lane = lax.broadcasted_iota(jnp.int32, (8, TILE), 1)
            query = (lane + at) % HALF + jnp.where(is_a, 0, HALF)
            limit = query - sub * SEG
        if slow:
            p = jnp.ones((8, TILE), f32)
            for r in reversed(range(SEG)):
                beta = 1.0 / (1.0 + jnp.exp2(-z[r * 8:(r + 1) * 8, :]))
                if diag:
                    beta = jnp.where(r < limit, beta, 0.0)
                w = p * beta
                p = p - w
                wts[r * 8:(r + 1) * 8, here] = w
            e = exclusive(p)
            total = e[0:1, :] * p[0:1, :]
            e = e * start
            scales = [e] * (SEG // CHUNK)
        else:
            ends, good = [], None
            for ch in range(SEG // CHUNK):
                f = jnp.ones((8, TILE), f32)
                for r in range(ch * CHUNK, (ch + 1) * CHUNK):
                    x = jnp.exp2(z[r * 8:(r + 1) * 8, :])
                    if diag:
                        x = jnp.where(r < limit, x, 0.0)
                    w = x * f
                    f = f + w
                    wts[r * 8:(r + 1) * 8, here] = w
                fine = jnp.where(f < 1e36, 1.0, 0.0)
                good = fine if good is None else jnp.minimum(good, fine)
                ends.append(1.0 / f)
            okay[:, here] = jnp.minimum(okay[:, here], good)
            p = ends[0] * ends[1] * ends[2]
            e = exclusive(p)
            total = e[0:1, :] * p[0:1, :]
            e = e * start
            s2 = e * ends[2]
            s1 = s2 * ends[1]
            scales = [s1 * ends[0], s1, s2]
        both = [jnp.concatenate([s, s], axis=0) for s in scales]
        parts = []
        for r in range(0, SEG, 2):
            parts.append((wts[r * 8:(r + 2) * 8, here] * both[r // CHUNK]).astype(bf16))
        weight = jnp.concatenate(parts, axis=0)
        return start * total, jnp.dot(vt[...], weight, preferred_element_type=f32)

    def tiles(half, is_a, diag, slow):
        spots = range(0, COLS, TILE)
        starts = [carry[half, :, at:at + TILE] for at in spots]
        done = [tile(half, at, is_a, diag, slow, start) for at, start in zip(spots, starts)]
        for at, (left, added) in zip(spots, done):
            carry[half, :, at:at + TILE] = left
            acc[half, :, at:at + TILE] += added

    def sweep(slow):
        acc[...] = jnp.zeros_like(acc)
        carry[...] = jnp.ones_like(carry)

        def step(s, c):
            is_a = s <= i
            block = jnp.where(is_a, i - s, n - s)
            half = jnp.where(is_a, 0, 1)
            rows = kv_ref[block, 0:BLK, :]
            lk[:, 0:128] = rows
            wide = rows.astype(f32)
            turned = pltpu.roll(wide, 64, 1)
            logit = kv_ref[block, BLK:BLK + 8, :].astype(f32)
            lane = lax.broadcasted_iota(jnp.int32, (128, 128), 1)
            for j in range(3):
                column = jnp.broadcast_to(logit[j:j + 1, :], (128, 128)).T
                side = jnp.where(lane < 2, column, jnp.where(lane < 5, 1.0, jnp.where(lane < 64, 0.0, turned[j * 128:(j + 1) * 128, :])))
                lk[j * 128:(j + 1) * 128, 128:256] = side.astype(bf16)
            vt[...] = wide.T[64:128, :].astype(bf16)
            edge = jnp.logical_or(s == 0, s == i + 1)

            @pl.when(edge)
            def _():
                tiles(half, is_a, True, slow)

            @pl.when(jnp.logical_not(edge))
            def _():
                tiles(half, is_a, False, slow)
            return c

        lax.fori_loop(0, n + 1, step, 0)

    okay[...] = jnp.ones_like(okay)
    sweep(False)

    @pl.when(jnp.min(okay[...]) < 0.5)
    def _():
        sweep(True)

    stacked = jnp.concatenate([acc[0], acc[1]], axis=0).T
    for s in range(2):
        heads = [stacked[h * HALF:(h + 1) * HALF, s * 64:(s + 1) * 64] for h in range(HEADS)]
        out_ref[s * HALF:(s + 1) * HALF, :] = jnp.concatenate(heads, axis=1).astype(bf16)


def attention(n, position, kv, q, offsets):
    vm = pl.BlockSpec(memory_space=pltpu.VMEM)
    sm = pl.BlockSpec(memory_space=pltpu.SMEM)
    return pl.pallas_call(
        functools.partial(attention_kernel, n),
        out_shape=jax.ShapeDtypeStruct((BLK, HEADS * HEAD_DIM), jnp.bfloat16),
        in_specs=[sm, vm, vm, sm],
        out_specs=vm,
        scratch_shapes=[
            pltpu.VMEM((2, 256, COLS), jnp.bfloat16),
            pltpu.VMEM((BLK, 256), jnp.bfloat16),
            pltpu.VMEM((64, BLK), jnp.bfloat16),
            pltpu.VMEM((2, 64, COLS), jnp.float32),
            pltpu.VMEM((2, 8, COLS), jnp.float32),
            pltpu.VMEM((8, COLS), jnp.float32),
            pltpu.VMEM((BLK, COLS), jnp.float32),
        ],
        compiler_params=pltpu.CompilerParams(vmem_limit_bytes=40 * 1024 * 1024),
        name="attention",
    )(position, kv, q, offsets)


ROWS = 400
CUT = 192
MESH = pl.DeviceIdType.MESH


def gather_kernel(n, k_ref, v_ref, l_ref, q_ref, kv_ref, qs_ref, send, recv):
    f32, bf16 = jnp.float32, jnp.bfloat16
    me = lax.axis_index("sp")
    z, y, core = me // 8, (me // 2) % 4, me % 2

    def at(a, b, c):
        dz, dy = a * c + b * (1 - c), a * (1 - c) + b * c
        return ((z + dz + 4) % 4) * 8 + ((y + dy + 4) % 4) * 2 + c

    other, mirror = me + 1 - 2 * core, n - 1 - me
    near = [at(1, 0, core), at(3, 0, core)], [at(0, 1, core), at(0, 3, core)]
    barrier = pltpu.get_barrier_semaphore()
    for peer in near[0] + near[1] + [other, mirror]:
        pl.semaphore_signal(barrier, inc=1, device_id={"sp": peer}, device_id_type=MESH)

    spot = lax.broadcasted_iota(jnp.int32, (BLK, BLK), 0)
    source = lax.broadcasted_iota(jnp.int32, (BLK, BLK), 1)
    order = jnp.where(source == (spot % 8) * SEG + spot // 8, 1.0, 0.0).astype(bf16)
    both = jnp.concatenate([k_ref[...], v_ref[...]], axis=1)
    kv_ref[me, 0:BLK, :] = jnp.dot(order, both, preferred_element_type=f32).astype(bf16)
    logit = jnp.broadcast_to(l_ref[...].astype(f32), (BLK, 128)).astype(bf16)
    logit = jnp.dot(order, logit, preferred_element_type=f32)
    row = lax.broadcasted_iota(jnp.int32, (16, 128), 0)
    tail = jnp.zeros((16, 128), f32)
    for j in range(3):
        tail = jnp.where(row == j, logit[j * 128:(j + 1) * 128, :].T[0:16, :], tail)
    kv_ref[me, BLK:ROWS, :] = tail.astype(bf16)
    qs_ref[0:HALF, :] = q_ref[0:HALF, :]
    pl.semaphore_wait(barrier, 6)

    begun = []
    parts = (slice(0, ROWS), slice(0, CUT), slice(CUT, ROWS))

    def copy(index, slot, part, peer):
        piece = kv_ref.at[slot, parts[part]]
        return pltpu.make_async_remote_copy(
            src_ref=piece, dst_ref=piece, send_sem=send.at[index], recv_sem=recv.at[index],
            device_id={"sp": peer}, device_id_type=MESH)

    def begin(index, slot, part, peer):
        c = copy(index, slot, part, peer)
        c.start()
        begun.append(c)

    def arrive(index, slot, part):
        copy(index, slot, part, me).wait_recv()

    around = (0, 3, 1, 2)

    def spread(k, a):
        slot = at(a, 0, core)
        for d in range(2):
            begin(4 + 4 * k + d, slot, 0, near[1][d])
        begin(20 + k, slot, 0, other)

    swap = pltpu.make_async_remote_copy(
        src_ref=q_ref.at[HALF:BLK], dst_ref=qs_ref.at[HALF:BLK], send_sem=send.at[36], recv_sem=recv.at[36],
        device_id={"sp": mirror}, device_id_type=MESH)
    for d in range(2):
        begin(d, me, 0, near[0][d])
    spread(0, 0)
    swap.start()
    for d, a in ((0, 3), (1, 1)):
        slot = at(a, 0, core)
        arrive(d, slot, 0)
        begin(2 + d, slot, 1 + d, near[0][d])
        spread(1 + d, a)
    for k, a in enumerate(around):
        if k == 3:
            slot = at(2, 0, core)
            for d in range(2):
                arrive(2 + d, slot, 1 + d)
            spread(3, 2)
        for d, b in ((0, 3), (1, 1)):
            slot = at(a, b, core)
            arrive(4 + 4 * k + d, slot, 0)
            begin(6 + 4 * k + d, slot, 1 + d, near[1][d])
            begin(24 + 4 * d + k, slot, 0, other)
    for k, a in enumerate(around):
        slot = at(a, 2, core)
        for d in range(2):
            arrive(6 + 4 * k + d, slot, 1 + d)
        begin(32 + k, slot, 0, other)
    for j, b in enumerate((0, 3, 1, 2)):
        for k, a in enumerate(around):
            arrive(20 + 4 * j + k, at(a, b, 1 - core), 0)
    swap.wait_recv()
    for c in begun:
        c.wait_send()
    swap.wait_send()


def gather(n, k, v, logit, q):
    vm = pl.BlockSpec(memory_space=pltpu.VMEM)
    return pl.pallas_call(
        functools.partial(gather_kernel, n),
        out_shape=(
            jax.ShapeDtypeStruct((n, ROWS, 128), jnp.bfloat16),
            jax.ShapeDtypeStruct((BLK, HEADS * HEAD_DIM), jnp.bfloat16),
        ),
        in_specs=[vm] * 4,
        out_specs=(vm, vm),
        scratch_shapes=[pltpu.SemaphoreType.DMA((37,)), pltpu.SemaphoreType.DMA((37,))],
        compiler_params=pltpu.CompilerParams(collective_id=0, has_side_effects=True, vmem_limit_bytes=24 * 1024 * 1024),
        name="gather",
    )(k, v, logit, q)


WIDTH = 2048
FF_WIDTH = 1024
OWN = 96
CAP = 3
LANES = 128


def moe_kernel(n_sp, n_tp, halves, stream, wo_hbm, gain, aux, wg_hbm, wu_hbm, wd_hbm, out_ref,
               wo, wg, wu, wd, heads, mixed, normed, wide, going, coming, back, rows, hidden, pick,
               load, sends, recvs, bulk):
    f32, bf16 = jnp.float32, jnp.bfloat16
    n = n_sp * n_tp
    slots = n * CAP
    fold = WIDTH // LANES
    unit = CAP * fold
    sp, tp = lax.axis_index("sp"), lax.axis_index("tp")
    me = sp * n_tp + tp
    z, y, core = sp // 8, (sp // 2) % 4, sp % 2
    mirror = n_sp - 1 - sp

    def peer(o):
        x2 = (tp + o) % 4
        y2 = (y + o // 4) % 4
        z2 = (z + o // 16) % 4
        c2 = (core + o // 64) % 2
        return z2 * 8 + y2 * 2 + c2, x2

    barrier = pltpu.get_barrier_semaphore()

    def greet(o, c):
        s2, x2 = peer(o)
        pl.semaphore_signal(barrier, inc=1, device_id={"sp": s2, "tp": x2}, device_id_type=MESH)
        return c

    lax.fori_loop(1, n, greet, 0)
    loads = [pltpu.make_async_copy(wo_hbm, wo, load.at[0]), pltpu.make_async_copy(wg_hbm.at[0], wg, load.at[1]),
             pltpu.make_async_copy(wu_hbm.at[0], wu, load.at[2]), pltpu.make_async_copy(wd_hbm.at[0], wd, load.at[3])]
    for c in loads:
        c.start()

    lane = lax.broadcasted_iota(jnp.int32, (OWN, n), 1).astype(f32)
    below = lax.broadcasted_iota(jnp.int32, (OWN, OWN), 0) > lax.broadcasted_iota(jnp.int32, (OWN, OWN), 1)
    below = jnp.where(below, 1.0, 0.0).astype(bf16)
    place = lax.broadcasted_iota(jnp.int32, (OWN, slots), 1).astype(f32)
    ahead = jnp.zeros((1, n), f32)
    for k in range(2):
        ids = aux[:, k:k + 1]
        hit = jnp.where(lane == ids, 1.0, 0.0)
        before = jnp.dot(below, hit.astype(bf16), preferred_element_type=f32) + ahead
        rank = jnp.sum(hit * before, axis=1, keepdims=True)
        ahead = ahead + jnp.sum(hit, axis=0, keepdims=True)
        pick[k] = jnp.where(place == ids * CAP + rank, 1.0, 0.0).astype(bf16)

    pl.semaphore_wait(barrier, n - 1)

    def piece(j, source):
        return pltpu.make_async_remote_copy(
            src_ref=halves.at[j * OWN:(j + 1) * OWN], dst_ref=heads.at[source], send_sem=sends.at[j], recv_sem=recvs.at[source],
            device_id={"sp": sp if j < 2 else mirror, "tp": j}, device_id_type=MESH)

    for j in range(4):
        if j < 2:
            @pl.when(tp == j)
            def _():
                heads[j] = halves[j * OWN:(j + 1) * OWN, :]

            @pl.when(tp != j)
            def _():
                piece(j, tp).start()
        else:
            piece(j, tp).start()
    for p in range(4):
        if p < 2:
            @pl.when(tp != p)
            def _():
                piece(p, p).wait_recv()
        else:
            piece(p, p).wait_recv()

    loads[0].wait()
    every = jnp.concatenate([heads[p] for p in range(4)], axis=1)
    square = jnp.zeros((OWN, 1), f32)
    for at in range(0, WIDTH, 512):
        here = slice(at, at + 512)
        part = stream[:, here].astype(f32) + jnp.dot(every, wo[:, here], preferred_element_type=f32)
        part = part.astype(bf16)
        mixed[:, here] = part
        part = part.astype(f32)
        square = square + jnp.sum(part * part, axis=1, keepdims=True)
    factor = lax.rsqrt(square / WIDTH + norm_eps)
    normed[...] = (mixed[...].astype(f32) * factor * gain[...]).astype(bf16)

    def narrow(target):
        def one(b, c):
            span = pl.ds(pl.multiple_of(b * 256, 256), 256)
            target[span, :] = wide[span, :].astype(bf16)
            return c
        lax.fori_loop(0, slots * fold // 256, one, 0)

    def unfold(source):
        def one(b, c):
            span = pl.ds(pl.multiple_of(b * 256, 256), 256)
            wide[span, :] = source[span, :].astype(f32)
            return c
        lax.fori_loop(0, slots * fold // 256, one, 0)
        for c in range(fold):
            rows[:, c * LANES:(c + 1) * LANES] = wide[pl.ds(c, slots, stride=fold), :].astype(bf16)

    def store(at, value):
        for c in range(value.shape[1] // LANES):
            wide[pl.ds(at + c, slots, stride=fold), :] = value[:, c * LANES:(c + 1) * LANES]

    def span_of(d):
        return pl.ds(pl.multiple_of(d * unit, unit), unit)

    def exchange(source, target, k):
        def one(o, c):
            s2, x2 = peer(o)
            pltpu.make_async_remote_copy(
                src_ref=source.at[span_of(s2 * n_tp + x2)], dst_ref=target.at[span_of(me)], send_sem=bulk.at[k], recv_sem=bulk.at[k + 1],
                device_id={"sp": s2, "tp": x2}, device_id_type=MESH).start()
            return c

        lax.fori_loop(1, n, one, 0)
        target[span_of(me), :] = source[span_of(me), :]
        most = pl.ds(0, (n - 1) * unit)
        whole = pltpu.make_async_remote_copy(
            src_ref=source.at[most], dst_ref=target.at[most], send_sem=bulk.at[k], recv_sem=bulk.at[k + 1],
            device_id={"sp": mirror, "tp": tp}, device_id_type=MESH)
        whole.wait_recv()
        return whole

    chooser = (pick[0] + pick[1]).astype(f32).T.astype(bf16)
    for at in range(0, WIDTH, 256):
        store(at // LANES, jnp.dot(chooser, normed[:, at:at + 256], preferred_element_type=f32))
    narrow(going)
    first = exchange(going, coming, 0)
    unfold(coming)
    loads[1].wait()
    loads[2].wait()

    def up(b, c):
        here = pl.ds(pl.multiple_of(b * 256, 256), 256)
        gated = jnp.dot(rows[...], wg[:, here], preferred_element_type=f32)
        raised = jnp.dot(rows[...], wu[:, here], preferred_element_type=f32)
        hidden[:, here] = (gated / (1.0 + jnp.exp(-gated)) * raised).astype(bf16)
        return c

    lax.fori_loop(0, FF_WIDTH // 256, up, 0)
    loads[3].wait()
    first.wait_send()
    for at in range(0, WIDTH, 256):
        store(at // LANES, jnp.dot(hidden[...], wd[:, at:at + 256], preferred_element_type=f32))
    narrow(going)
    second = exchange(going, back, 2)
    unfold(back)

    high = jnp.maximum(aux[:, 2:3], aux[:, 3:4])
    e0, e1 = jnp.exp(aux[:, 2:3] - high), jnp.exp(aux[:, 3:4] - high)
    scale = 1.0 / (1.0 + jnp.exp(-aux[:, 4:5])) / (e0 + e1)
    for at in range(0, WIDTH, 256):
        here = slice(at, at + 256)
        total = jnp.dot(pick[0], rows[:, here], preferred_element_type=f32) * (scale * e0)
        total = total + jnp.dot(pick[1], rows[:, here], preferred_element_type=f32) * (scale * e1)
        out_ref[:, here] = (mixed[:, here].astype(f32) + total).astype(bf16)
    second.wait_send()
    for j in range(4):
        if j < 2:
            @pl.when(tp != j)
            def _():
                piece(j, tp).wait_send()
        else:
            piece(j, tp).wait_send()


def moe(n_sp, n_tp, halves, stream, out_weight, gain, aux, gate, up, down):
    vm = pl.BlockSpec(memory_space=pltpu.VMEM)
    hbm = pl.BlockSpec(memory_space=pl.ANY)
    slots = n_sp * n_tp * CAP
    linear = (slots * WIDTH // LANES, LANES)
    bf16 = jnp.bfloat16
    dma = pltpu.SemaphoreType.DMA
    return pl.pallas_call(
        functools.partial(moe_kernel, n_sp, n_tp),
        out_shape=jax.ShapeDtypeStruct((OWN, WIDTH), bf16),
        in_specs=[vm, vm, hbm, vm, vm, hbm, hbm, hbm],
        out_specs=vm,
        scratch_shapes=[
            pltpu.VMEM((1024, WIDTH), bf16), pltpu.VMEM((WIDTH, FF_WIDTH), bf16), pltpu.VMEM((WIDTH, FF_WIDTH), bf16), pltpu.VMEM((FF_WIDTH, WIDTH), bf16),
            pltpu.VMEM((4, OWN, 256), bf16), pltpu.VMEM((OWN, WIDTH), bf16), pltpu.VMEM((OWN, WIDTH), bf16),
            pltpu.VMEM(linear, jnp.float32), pltpu.VMEM(linear, bf16), pltpu.VMEM(linear, bf16), pltpu.VMEM(linear, bf16),
            pltpu.VMEM((slots, WIDTH), bf16), pltpu.VMEM((slots, FF_WIDTH), bf16), pltpu.VMEM((2, OWN, slots), bf16),
            dma((4,)), dma((4,)), dma((4,)), dma((4,)),
        ],
        compiler_params=pltpu.CompilerParams(collective_id=1, has_side_effects=True, vmem_limit_bytes=56 * 1024 * 1024),
        name="experts",
    )(halves, stream, out_weight, gain, aux, gate, up, down)


def on_device(
    queries,
    key_rows,
    value_rows,
    key_logit,
    head_offset,
    stream,
    out_weight,
    norm_gain,
    expert_ids,
    group_logit,
    expert_logits,
    gate_weight,
    up_weight,
    down_weight,
):
    n_sp, n_tp = lax.axis_size("sp"), lax.axis_size("tp")
    position = lax.axis_index("sp").astype(jnp.int32).reshape(1)
    kv, chosen = gather(n_sp, key_rows, value_rows, key_logit, queries)
    halves = attention(n_sp, position, kv, chosen, head_offset)
    aux = jnp.concatenate([expert_ids.astype(jnp.float32), expert_logits, group_logit[:, None]], axis=1)
    return moe(n_sp, n_tp, halves, stream, out_weight, norm_gain[None], aux, gate_weight, up_weight, down_weight)


def solution(mesh):
    placed = (
        P("sp", "tp"),
        P("sp", "tp"),
        P("sp", "tp"),
        P("sp", "tp"),
        P("tp"),
        P(("sp", "tp"), None),
        P(),
        P(),
        P(("sp", "tp"), None),
        P(("sp", "tp")),
        P(("sp", "tp"), None),
        P(("sp", "tp"), None, None),
        P(("sp", "tp"), None, None),
        P(("sp", "tp"), None, None),
    )
    return jax.shard_map(
        on_device, mesh=mesh, in_specs=placed, out_specs=P(("sp", "tp"), None), check_vma=False
    )
```

```python
import functools

import jax
import jax.numpy as jnp
from jax import lax
from jax.experimental import pallas as pl
from jax.experimental.pallas import tpu as pltpu
from jax.sharding import PartitionSpec as P

HEAD_DIM = 64
norm_eps = 1e-06
HEADS = 4
BLK = 384
HALF = 192
SEG = 48
CHUNK = 16
COLS = 768
TILE = 256
LOG2E = 1.4426950408889634


def split3(x):
    hi = x.astype(jnp.bfloat16).astype(jnp.float32)
    rest = x - hi
    mid = rest.astype(jnp.bfloat16).astype(jnp.float32)
    lo = (rest - mid).astype(jnp.bfloat16).astype(jnp.float32)
    return hi, mid, lo


def attention_kernel(n, pos_ref, kv_ref, q_ref, off_ref, out_ref, qt, lk, vt, acc, carry, okay, wts, z0, z1):
    i = pos_ref[0]
    za = (z0, z1)
    f32, bf16 = jnp.float32, jnp.bfloat16
    for s in range(2):
        qs = q_ref[s * HALF:(s + 1) * HALF, :].astype(f32) * (LOG2E * HEAD_DIM ** -0.5)
        rows = jnp.concatenate([qs[:, h * 64:(h + 1) * 64] for h in range(HEADS)], axis=0)
        high = rows.astype(bf16).astype(f32)
        low = rows - high
        zero = jnp.zeros_like(rows)
        top = jnp.concatenate([high, zero], axis=1).T
        bottom = jnp.concatenate([zero, low], axis=1).T
        lane = lax.broadcasted_iota(jnp.int32, (8, COLS), 1)
        off = jnp.zeros((8, COLS), f32)
        for h in range(HEADS):
            inside = jnp.logical_and(lane >= h * HALF, lane < (h + 1) * HALF)
            off = jnp.where(inside, off_ref[h] * LOG2E, off)
        hi, mid, lo = split3(off)
        row = lax.broadcasted_iota(jnp.int32, (8, COLS), 0)
        c_hi = 1.4453125
        extra = jnp.where(row == 0, c_hi, jnp.where(row == 1, LOG2E - c_hi, jnp.where(row == 2, hi, jnp.where(row == 3, mid, jnp.where(row == 4, lo, 0.0)))))
        bottom = jnp.concatenate([extra, bottom[8:, :]], axis=0)
        qt[s, 0:128, :] = top.astype(bf16)
        qt[s, 128:256, :] = bottom.astype(bf16)

    sub = lax.broadcasted_iota(jnp.int32, (8, TILE), 0)

    def exclusive(p):
        e = jnp.where(sub == 7, 1.0, pltpu.roll(p, 7, 0))
        e = e * jnp.where(sub == 7, 1.0, pltpu.roll(e, 7, 0))
        e = e * jnp.where(sub >= 6, 1.0, pltpu.roll(e, 6, 0))
        e = e * jnp.where(sub >= 4, 1.0, pltpu.roll(e, 4, 0))
        return e

    def tile(zs, at, row, slow, start):
        here = slice(at, at + TILE)
        if row is not None:
            lane = lax.broadcasted_iota(jnp.int32, (8, TILE), 1)
            limit = (lane + at) % HALF + row - sub * SEG
        if slow:
            p = jnp.ones((8, TILE), f32)
            for r in reversed(range(SEG)):
                beta = 1.0 / (1.0 + jnp.exp2(-zs[r * 8:(r + 1) * 8, here]))
                if row is not None:
                    beta = jnp.where(r < limit, beta, 0.0)
                w = p * beta
                p = p - w
                wts[r * 8:(r + 1) * 8, here] = w
            e = exclusive(p)
            total = e[0:1, :] * p[0:1, :]
            e = e * start
            scales = [e] * (SEG // CHUNK)
        else:
            ends, good = [], None
            for ch in range(SEG // CHUNK):
                f = jnp.ones((8, TILE), f32)
                for r in range(ch * CHUNK, (ch + 1) * CHUNK):
                    x = jnp.exp2(zs[r * 8:(r + 1) * 8, here])
                    if row is not None:
                        x = jnp.where(r < limit, x, 0.0)
                    w = x * f
                    f = f + w
                    wts[r * 8:(r + 1) * 8, here] = w
                fine = jnp.where(f < 1e36, 1.0, 0.0)
                good = fine if good is None else jnp.minimum(good, fine)
                ends.append(1.0 / f)
            okay[:, here] = jnp.minimum(okay[:, here], good)
            p = ends[0] * ends[1] * ends[2]
            e = exclusive(p)
            total = e[0:1, :] * p[0:1, :]
            e = e * start
            s2 = e * ends[2]
            s1 = s2 * ends[1]
            scales = [s1 * ends[0], s1, s2]
        both = [jnp.concatenate([s, s], axis=0) for s in scales]
        parts = []
        for r in range(0, SEG, 2):
            parts.append((wts[r * 8:(r + 2) * 8, here] * both[r // CHUNK]).astype(bf16))
        return start * total, jnp.concatenate(parts, axis=0)

    spots = range(0, COLS, TILE)

    def load(block, k):
        rows = kv_ref[block, 0:BLK, :]
        lk[k, :, 0:128] = rows
        wide = rows.astype(f32)
        turned = pltpu.roll(wide, 64, 1)
        logit = kv_ref[block, BLK:BLK + 8, :].astype(f32)
        lane = lax.broadcasted_iota(jnp.int32, (128, 128), 1)
        for j in range(3):
            column = jnp.broadcast_to(logit[j:j + 1, :], (128, 128)).T
            side = jnp.where(lane < 2, column, jnp.where(lane < 5, 1.0, jnp.where(lane < 64, 0.0, turned[j * 128:(j + 1) * 128, :])))
            lk[k, j * 128:(j + 1) * 128, 128:256] = side.astype(bf16)
        vt[k] = wide.T[64:128, :].astype(bf16)

    def score(half, k, at):
        za[k][:, at:at + TILE] = jnp.dot(lk[k], qt[half, :, at:at + TILE], preferred_element_type=f32)

    def process(half, k, row, slow, after=None):
        starts = [carry[half, :, at:at + TILE] for at in spots]
        for at, start in zip(spots, starts):
            if after is not None:
                score(after, 1 - k, at)
            left, weight = tile(za[k], at, row, slow, start)
            carry[half, :, at:at + TILE] = left
            acc[half, :, at:at + TILE] += jnp.dot(vt[k], weight, preferred_element_type=f32)

    def sweep(slow):
        acc[...] = jnp.zeros_like(acc)
        carry[...] = jnp.ones_like(carry)
        for half, block in ((0, i), (1, n - 1 - i)):
            load(block, 0)
            for at in spots:
                score(half, 0, at)
            process(half, 0, HALF * half, slow)

        def which(s):
            return jnp.where(s < i, 0, 1), jnp.maximum(jnp.where(s < i, i - 1 - s, n - 2 - s), 0)

        half, block = which(0)
        load(block, 0)
        for at in spots:
            score(half, 0, at)

        def pair(t, c):
            for k in range(2):
                half, block = which(2 * t + k)
                after, block = which(2 * t + k + 1)
                load(block, 1 - k)
                process(half, k, None, slow, after)
            return c

        lax.fori_loop(0, (n - 2) // 2, pair, 0)
        process(which(n - 2)[0], 0, None, slow)

    okay[...] = jnp.ones_like(okay)
    sweep(False)

    @pl.when(jnp.min(okay[...]) < 0.5)
    def _():
        sweep(True)

    stacked = jnp.concatenate([acc[0], acc[1]], axis=0).T
    for s in range(2):
        heads = [stacked[h * HALF:(h + 1) * HALF, s * 64:(s + 1) * 64] for h in range(HEADS)]
        out_ref[s * HALF:(s + 1) * HALF, :] = jnp.concatenate(heads, axis=1).astype(bf16)


def attention(n, position, kv, q, offsets):
    vm = pl.BlockSpec(memory_space=pltpu.VMEM)
    sm = pl.BlockSpec(memory_space=pltpu.SMEM)
    return pl.pallas_call(
        functools.partial(attention_kernel, n),
        out_shape=jax.ShapeDtypeStruct((BLK, HEADS * HEAD_DIM), jnp.bfloat16),
        in_specs=[sm, vm, vm, sm],
        out_specs=vm,
        scratch_shapes=[
            pltpu.VMEM((2, 256, COLS), jnp.bfloat16),
            pltpu.VMEM((2, BLK, 256), jnp.bfloat16),
            pltpu.VMEM((2, 64, BLK), jnp.bfloat16),
            pltpu.VMEM((2, 64, COLS), jnp.float32),
            pltpu.VMEM((2, 8, COLS), jnp.float32),
            pltpu.VMEM((8, COLS), jnp.float32),
            pltpu.VMEM((BLK, COLS), jnp.float32),
            pltpu.VMEM((BLK, COLS), jnp.float32),
            pltpu.VMEM((BLK, COLS), jnp.float32),
        ],
        compiler_params=pltpu.CompilerParams(vmem_limit_bytes=40 * 1024 * 1024),
        name="attention",
    )(position, kv, q, offsets)


ROWS = 400
CUT = 192
MESH = pl.DeviceIdType.MESH


def gather_kernel(n, k_ref, v_ref, l_ref, q_ref, kv_ref, qs_ref, send, recv):
    f32, bf16 = jnp.float32, jnp.bfloat16
    me = lax.axis_index("sp")
    z, y, core = me // 8, (me // 2) % 4, me % 2

    def at(a, b, c):
        dz, dy = a * c + b * (1 - c), a * (1 - c) + b * c
        return ((z + dz + 4) % 4) * 8 + ((y + dy + 4) % 4) * 2 + c

    other, mirror = me + 1 - 2 * core, n - 1 - me
    near = [at(1, 0, core), at(3, 0, core)], [at(0, 1, core), at(0, 3, core)]
    barrier = pltpu.get_barrier_semaphore()
    for peer in near[0] + near[1] + [other, mirror]:
        pl.semaphore_signal(barrier, inc=1, device_id={"sp": peer}, device_id_type=MESH)

    spot = lax.broadcasted_iota(jnp.int32, (BLK, BLK), 0)
    source = lax.broadcasted_iota(jnp.int32, (BLK, BLK), 1)
    order = jnp.where(source == (spot % 8) * SEG + spot // 8, 1.0, 0.0).astype(bf16)
    across = (((1,), (1,)), ((), ()))
    both = jnp.concatenate([k_ref[...], v_ref[...]], axis=0)
    kv_ref[me, 0:BLK, :] = lax.dot_general(order, both, across, preferred_element_type=f32).astype(bf16)
    logit = jnp.broadcast_to(l_ref[...].astype(f32), (16, BLK)).astype(bf16)
    logit = lax.dot_general(logit, order, across, preferred_element_type=f32)
    row = lax.broadcasted_iota(jnp.int32, (16, 128), 0)
    tail = jnp.zeros((16, 128), f32)
    for j in range(3):
        tail = jnp.where(row == j, logit[:, j * 128:(j + 1) * 128], tail)
    kv_ref[me, BLK:ROWS, :] = tail.astype(bf16)
    qs_ref[0:HALF, :] = q_ref[0:HALF, :]
    pl.semaphore_wait(barrier, 6)

    begun = []
    parts = (slice(0, ROWS), slice(0, CUT), slice(CUT, ROWS))

    def copy(index, slot, part, peer):
        piece = kv_ref.at[slot, parts[part]]
        return pltpu.make_async_remote_copy(
            src_ref=piece, dst_ref=piece, send_sem=send.at[index], recv_sem=recv.at[index],
            device_id={"sp": peer}, device_id_type=MESH)

    def begin(index, slot, part, peer):
        c = copy(index, slot, part, peer)
        c.start()
        begun.append(c)

    def arrive(index, slot, part):
        copy(index, slot, part, me).wait_recv()

    around = (0, 3, 1, 2)

    def spread(k, a):
        slot = at(a, 0, core)
        for d in range(2):
            begin(4 + 4 * k + d, slot, 0, near[1][d])
        begin(20 + k, slot, 0, other)

    swap = pltpu.make_async_remote_copy(
        src_ref=q_ref.at[HALF:BLK], dst_ref=qs_ref.at[HALF:BLK], send_sem=send.at[36], recv_sem=recv.at[36],
        device_id={"sp": mirror}, device_id_type=MESH)
    for d in range(2):
        begin(d, me, 0, near[0][d])
    spread(0, 0)
    swap.start()
    for d, a in ((0, 3), (1, 1)):
        slot = at(a, 0, core)
        arrive(d, slot, 0)
        begin(2 + d, slot, 1 + d, near[0][d])
        spread(1 + d, a)
    for k, a in enumerate(around):
        if k == 3:
            slot = at(2, 0, core)
            for d in range(2):
                arrive(2 + d, slot, 1 + d)
            spread(3, 2)
        for d, b in ((0, 3), (1, 1)):
            slot = at(a, b, core)
            arrive(4 + 4 * k + d, slot, 0)
            begin(6 + 4 * k + d, slot, 1 + d, near[1][d])
            begin(24 + 4 * d + k, slot, 0, other)
    for k, a in enumerate(around):
        slot = at(a, 2, core)
        for d in range(2):
            arrive(6 + 4 * k + d, slot, 1 + d)
        begin(32 + k, slot, 0, other)
    for j, b in enumerate((0, 3, 1, 2)):
        for k, a in enumerate(around):
            arrive(20 + 4 * j + k, at(a, b, 1 - core), 0)
    swap.wait_recv()
    for c in begun:
        c.wait_send()
    swap.wait_send()


def gather(n, k, v, logit, q):
    vm = pl.BlockSpec(memory_space=pltpu.VMEM)
    return pl.pallas_call(
        functools.partial(gather_kernel, n),
        out_shape=(
            jax.ShapeDtypeStruct((n, ROWS, 128), jnp.bfloat16),
            jax.ShapeDtypeStruct((BLK, HEADS * HEAD_DIM), jnp.bfloat16),
        ),
        in_specs=[vm] * 4,
        out_specs=(vm, vm),
        scratch_shapes=[pltpu.SemaphoreType.DMA((37,)), pltpu.SemaphoreType.DMA((37,))],
        compiler_params=pltpu.CompilerParams(collective_id=0, has_side_effects=True, vmem_limit_bytes=24 * 1024 * 1024),
        name="gather",
    )(k, v, logit, q)


WIDTH = 2048
FF_WIDTH = 1024
OWN = 96
CAP = 3
LANES = 128


def moe_kernel(n_sp, n_tp, halves, stream, wo_hbm, gain, aux, wg_hbm, wu_hbm, wd_hbm, out_ref,
               wo, wg, wu, wd, heads, mixed, normed, wide, going, coming, leaving, back, rows, hidden, pick, total,
               load, sends, recvs, bulk):
    f32, bf16 = jnp.float32, jnp.bfloat16
    n = n_sp * n_tp
    groups = 4
    slots = n * CAP // groups
    fold = WIDTH // LANES
    unit = CAP * fold
    sp, tp = lax.axis_index("sp"), lax.axis_index("tp")
    me = sp * n_tp + tp
    z, y, core = sp // 8, (sp // 2) % 4, sp % 2
    mirror = n_sp - 1 - sp

    def peer(o):
        x2 = (tp + o) % 4
        y2 = (y + o // 4) % 4
        z2 = (z + o // 16) % 4
        c2 = (core + o // 64) % 2
        return z2 * 8 + y2 * 2 + c2, x2

    def member(g, s2):
        z2, y2 = s2 // 8, (s2 // 2) % 4
        return (g + tp + y + z - y2 - z2 + 8) % 4

    def source(g, s2):
        z2, y2 = s2 // 8, (s2 // 2) % 4
        return (tp + y + z - y2 - z2 - g + 12) % 4

    barrier = pltpu.get_barrier_semaphore()

    def greet(o, c):
        s2, x2 = peer(o)
        pl.semaphore_signal(barrier, inc=1, device_id={"sp": s2, "tp": x2}, device_id_type=MESH)
        return c

    lax.fori_loop(1, n, greet, 0)
    loads = [pltpu.make_async_copy(wo_hbm, wo, load.at[0]), pltpu.make_async_copy(wg_hbm.at[0], wg, load.at[1]),
             pltpu.make_async_copy(wu_hbm.at[0], wu, load.at[2]), pltpu.make_async_copy(wd_hbm.at[0], wd, load.at[3])]
    for c in loads:
        c.start()

    lane = lax.broadcasted_iota(jnp.int32, (OWN, n), 1).astype(f32)
    below = lax.broadcasted_iota(jnp.int32, (OWN, OWN), 0) > lax.broadcasted_iota(jnp.int32, (OWN, OWN), 1)
    below = jnp.where(below, 1.0, 0.0).astype(bf16)
    place = lax.broadcasted_iota(jnp.int32, (OWN, slots), 1)
    ahead = jnp.zeros((1, n), f32)
    for k in range(2):
        ids = aux[:, k:k + 1]
        hit = jnp.where(lane == ids, 1.0, 0.0)
        before = jnp.dot(below, hit.astype(bf16), preferred_element_type=f32) + ahead
        rank = jnp.sum(hit * before, axis=1, keepdims=True)
        ahead = ahead + jnp.sum(hit, axis=0, keepdims=True)
        whole = ids.astype(jnp.int32)
        spot = (whole >> 2) * CAP + rank.astype(jnp.int32)
        group = ((whole & 3) + ((whole >> 3) & 3) + (whole >> 5) - (tp + y + z) + 12) & 3
        for g in range(groups):
            pick[k, g] = jnp.where(jnp.logical_and(place == spot, group == g), 1.0, 0.0).astype(bf16)

    pl.semaphore_wait(barrier, n - 1)

    def piece(j, source):
        return pltpu.make_async_remote_copy(
            src_ref=halves.at[j * OWN:(j + 1) * OWN], dst_ref=heads.at[source], send_sem=sends.at[j], recv_sem=recvs.at[source],
            device_id={"sp": sp if j < 2 else mirror, "tp": j}, device_id_type=MESH)

    for j in range(4):
        if j < 2:
            @pl.when(tp == j)
            def _():
                heads[j] = halves[j * OWN:(j + 1) * OWN, :]

            @pl.when(tp != j)
            def _():
                piece(j, tp).start()
        else:
            piece(j, tp).start()
    for p in range(4):
        if p < 2:
            @pl.when(tp != p)
            def _():
                piece(p, p).wait_recv()
        else:
            piece(p, p).wait_recv()

    loads[0].wait()
    every = jnp.concatenate([heads[p] for p in range(4)], axis=1)
    square = jnp.zeros((OWN, 1), f32)
    for at in range(0, WIDTH, 512):
        here = slice(at, at + 512)
        part = stream[:, here].astype(f32) + jnp.dot(every, wo[:, here], preferred_element_type=f32)
        part = part.astype(bf16)
        mixed[:, here] = part
        part = part.astype(f32)
        square = square + jnp.sum(part * part, axis=1, keepdims=True)
    factor = lax.rsqrt(square / WIDTH + norm_eps)
    normed[...] = (mixed[...].astype(f32) * factor * gain[...]).astype(bf16)

    block = slots * fold

    def narrow(target, g):
        def one(b, c):
            span = pl.ds(pl.multiple_of(b * 256, 256), 256)
            target[g, span, :] = wide[span, :].astype(bf16)
            return c
        lax.fori_loop(0, block // 256, one, 0)

    def unfold(source, g):
        def one(b, c):
            span = pl.ds(pl.multiple_of(b * 256, 256), 256)
            wide[span, :] = source[g, span, :].astype(f32)
            return c
        lax.fori_loop(0, block // 256, one, 0)
        for c in range(fold):
            rows[:, c * LANES:(c + 1) * LANES] = wide[pl.ds(c, slots, stride=fold), :].astype(bf16)

    def store(at, value):
        for c in range(value.shape[1] // LANES):
            wide[pl.ds(at + c, slots, stride=fold), :] = value[:, c * LANES:(c + 1) * LANES]

    def span_of(d):
        return pl.ds(pl.multiple_of(d * unit, unit), unit)

    def send_group(origin, target, g, k, partner):
        def one(o, c):
            s2 = (sp + o) % n_sp
            pltpu.make_async_remote_copy(
                src_ref=origin.at[g, span_of(s2)], dst_ref=target.at[g, span_of(sp)], send_sem=bulk.at[k, g], recv_sem=bulk.at[k + 1, g],
                device_id={"sp": s2, "tp": partner(g, s2)}, device_id_type=MESH).start()
            return c

        lax.fori_loop(1 if g == 0 else 0, n_sp, one, 0)
        if g == 0:
            target[g, span_of(sp), :] = origin[g, span_of(sp), :]

    def rest(origin, target, g, k):
        most = pl.ds(0, (n_sp - 1 if g == 0 else n_sp) * unit)
        return pltpu.make_async_remote_copy(
            src_ref=origin.at[g, most], dst_ref=target.at[g, most], send_sem=bulk.at[k, g], recv_sem=bulk.at[k + 1, g],
            device_id={"sp": mirror, "tp": tp}, device_id_type=MESH)

    for g in range(groups):
        chooser = (pick[0, g] + pick[1, g]).astype(f32).T.astype(bf16)
        for at in range(0, WIDTH, 256):
            store(at // LANES, jnp.dot(chooser, normed[:, at:at + 256], preferred_element_type=f32))
        narrow(going, g)
        send_group(going, coming, g, 0, member)

    def up(b, c):
        here = pl.ds(pl.multiple_of(b * 256, 256), 256)
        gated = jnp.dot(rows[...], wg[:, here], preferred_element_type=f32)
        raised = jnp.dot(rows[...], wu[:, here], preferred_element_type=f32)
        hidden[:, here] = (gated / (1.0 + jnp.exp(-gated)) * raised).astype(bf16)
        return c

    for g in range(groups):
        rest(going, coming, g, 0).wait_recv()
        unfold(coming, g)
        if g == 0:
            loads[1].wait()
            loads[2].wait()
        lax.fori_loop(0, FF_WIDTH // 256, up, 0)
        if g == 0:
            loads[3].wait()
        for at in range(0, WIDTH, 256):
            store(at // LANES, jnp.dot(hidden[...], wd[:, at:at + 256], preferred_element_type=f32))
        narrow(leaving, g)
        send_group(leaving, back, g, 2, source)

    high = jnp.maximum(aux[:, 2:3], aux[:, 3:4])
    e0, e1 = jnp.exp(aux[:, 2:3] - high), jnp.exp(aux[:, 3:4] - high)
    scale = 1.0 / (1.0 + jnp.exp(-aux[:, 4:5])) / (e0 + e1)
    for g in range(groups):
        rest(leaving, back, g, 2).wait_recv()
        unfold(back, g)
        for at in range(0, WIDTH, 256):
            here = slice(at, at + 256)
            added = jnp.dot(pick[0, g], rows[:, here], preferred_element_type=f32) * (scale * e0)
            added = added + jnp.dot(pick[1, g], rows[:, here], preferred_element_type=f32) * (scale * e1)
            if g > 0:
                added = added + total[:, here]
            if g < groups - 1:
                total[:, here] = added
            else:
                out_ref[:, here] = (mixed[:, here].astype(f32) + added).astype(bf16)
    for g in range(groups):
        rest(going, coming, g, 0).wait_send()
        rest(leaving, back, g, 2).wait_send()
    for j in range(4):
        if j < 2:
            @pl.when(tp != j)
            def _():
                piece(j, tp).wait_send()
        else:
            piece(j, tp).wait_send()


def moe(n_sp, n_tp, halves, stream, out_weight, gain, aux, gate, up, down):
    vm = pl.BlockSpec(memory_space=pltpu.VMEM)
    hbm = pl.BlockSpec(memory_space=pl.ANY)
    groups = 4
    slots = n_sp * n_tp * CAP // groups
    linear = (slots * WIDTH // LANES, LANES)
    grouped = (groups,) + linear
    bf16 = jnp.bfloat16
    dma = pltpu.SemaphoreType.DMA
    return pl.pallas_call(
        functools.partial(moe_kernel, n_sp, n_tp),
        out_shape=jax.ShapeDtypeStruct((OWN, WIDTH), bf16),
        in_specs=[vm, vm, hbm, vm, vm, hbm, hbm, hbm],
        out_specs=vm,
        scratch_shapes=[
            pltpu.VMEM((1024, WIDTH), bf16), pltpu.VMEM((WIDTH, FF_WIDTH), bf16), pltpu.VMEM((WIDTH, FF_WIDTH), bf16), pltpu.VMEM((FF_WIDTH, WIDTH), bf16),
            pltpu.VMEM((4, OWN, 256), bf16), pltpu.VMEM((OWN, WIDTH), bf16), pltpu.VMEM((OWN, WIDTH), bf16),
            pltpu.VMEM(linear, jnp.float32),
            pltpu.VMEM(grouped, bf16), pltpu.VMEM(grouped, bf16), pltpu.VMEM(grouped, bf16), pltpu.VMEM(grouped, bf16),
            pltpu.VMEM((slots, WIDTH), bf16), pltpu.VMEM((slots, FF_WIDTH), bf16), pltpu.VMEM((2, groups, OWN, slots), bf16), pltpu.VMEM((OWN, WIDTH), jnp.float32),
            dma((4,)), dma((4,)), dma((4,)), dma((4, groups)),
        ],
        compiler_params=pltpu.CompilerParams(collective_id=1, has_side_effects=True, vmem_limit_bytes=56 * 1024 * 1024),
        name="experts",
    )(halves, stream, out_weight, gain, aux, gate, up, down)


def on_device(
    queries,
    key_rows,
    value_rows,
    key_logit,
    head_offset,
    stream,
    out_weight,
    norm_gain,
    expert_ids,
    group_logit,
    expert_logits,
    gate_weight,
    up_weight,
    down_weight,
):
    n_sp, n_tp = lax.axis_size("sp"), lax.axis_size("tp")
    position = lax.axis_index("sp").astype(jnp.int32).reshape(1)
    kv, chosen = gather(n_sp, key_rows.T, value_rows.T, key_logit.T, queries)
    halves = attention(n_sp, position, kv, chosen, head_offset)
    aux = jnp.concatenate([expert_ids.astype(jnp.float32), expert_logits, group_logit[:, None]], axis=1)
    return moe(n_sp, n_tp, halves, stream, out_weight, norm_gain[None], aux, gate_weight, up_weight, down_weight)


def solution(mesh):
    placed = (
        P("sp", "tp"),
        P("sp", "tp"),
        P("sp", "tp"),
        P("sp", "tp"),
        P("tp"),
        P(("sp", "tp"), None),
        P(),
        P(),
        P(("sp", "tp"), None),
        P(("sp", "tp")),
        P(("sp", "tp"), None),
        P(("sp", "tp"), None, None),
        P(("sp", "tp"), None, None),
        P(("sp", "tp"), None, None),
    )
    return jax.shard_map(
        on_device, mesh=mesh, in_specs=placed, out_specs=P(("sp", "tp"), None), check_vma=False
    )
```

```python
import functools

import jax
import jax.numpy as jnp
from jax import lax
from jax.experimental import pallas as pl
from jax.experimental.pallas import tpu as pltpu
from jax.sharding import PartitionSpec as P

HEAD_DIM = 64
norm_eps = 1e-06
HEADS = 4
BLK = 384
HALF = 192
SEG = 48
CHUNK = 16
COLS = 768
TILE = 768
LOG2E = 1.4426950408889634


def split3(x):
    hi = x.astype(jnp.bfloat16).astype(jnp.float32)
    rest = x - hi
    mid = rest.astype(jnp.bfloat16).astype(jnp.float32)
    lo = (rest - mid).astype(jnp.bfloat16).astype(jnp.float32)
    return hi, mid, lo


def attention_kernel(n, pos_ref, kv_ref, q_ref, off_ref, out_ref, qt, lk, vt, acc, carry, okay, wts, z0, z1):
    i = pos_ref[0]
    za = (z0, z1)
    f32, bf16 = jnp.float32, jnp.bfloat16
    for s in range(2):
        qs = q_ref[s * HALF:(s + 1) * HALF, :].astype(f32) * (LOG2E * HEAD_DIM ** -0.5)
        rows = jnp.concatenate([qs[:, h * 64:(h + 1) * 64] for h in range(HEADS)], axis=0)
        high = rows.astype(bf16).astype(f32)
        low = rows - high
        zero = jnp.zeros_like(rows)
        top = jnp.concatenate([high, zero], axis=1).T
        bottom = jnp.concatenate([zero, low], axis=1).T
        lane = lax.broadcasted_iota(jnp.int32, (8, COLS), 1)
        off = jnp.zeros((8, COLS), f32)
        for h in range(HEADS):
            inside = jnp.logical_and(lane >= h * HALF, lane < (h + 1) * HALF)
            off = jnp.where(inside, off_ref[h] * LOG2E, off)
        hi, mid, lo = split3(off)
        row = lax.broadcasted_iota(jnp.int32, (8, COLS), 0)
        c_hi = 1.4453125
        extra = jnp.where(row == 0, c_hi, jnp.where(row == 1, LOG2E - c_hi, jnp.where(row == 2, hi, jnp.where(row == 3, mid, jnp.where(row == 4, lo, 0.0)))))
        bottom = jnp.concatenate([extra, bottom[8:, :]], axis=0)
        qt[s, 0:128, :] = top.astype(bf16)
        qt[s, 128:256, :] = bottom.astype(bf16)

    sub = lax.broadcasted_iota(jnp.int32, (8, TILE), 0)

    def exclusive(p):
        e = jnp.where(sub == 7, 1.0, pltpu.roll(p, 7, 0))
        e = e * jnp.where(sub == 7, 1.0, pltpu.roll(e, 7, 0))
        e = e * jnp.where(sub >= 6, 1.0, pltpu.roll(e, 6, 0))
        e = e * jnp.where(sub >= 4, 1.0, pltpu.roll(e, 4, 0))
        return e

    def tile(zs, at, row, slow, start):
        here = slice(at, at + TILE)
        if row is not None:
            lane = lax.broadcasted_iota(jnp.int32, (8, TILE), 1)
            limit = (lane + at) % HALF + row - sub * SEG
        if slow:
            p = jnp.ones((8, TILE), f32)
            for r in reversed(range(SEG)):
                beta = 1.0 / (1.0 + jnp.exp2(-zs[r * 8:(r + 1) * 8, here]))
                if row is not None:
                    beta = jnp.where(r < limit, beta, 0.0)
                w = p * beta
                p = p - w
                wts[r * 8:(r + 1) * 8, here] = w
            e = exclusive(p)
            total = e[0:1, :] * p[0:1, :]
            e = e * start
            scales = [e] * (SEG // CHUNK)
        else:
            ends, good = [], None
            for ch in range(SEG // CHUNK):
                f = jnp.ones((8, TILE), f32)
                for r in range(ch * CHUNK, (ch + 1) * CHUNK):
                    x = jnp.exp2(zs[r * 8:(r + 1) * 8, here])
                    if row is not None:
                        x = jnp.where(r < limit, x, 0.0)
                    w = x * f
                    f = f + w
                    wts[r * 8:(r + 1) * 8, here] = w
                fine = jnp.where(f < 1e36, 1.0, 0.0)
                good = fine if good is None else jnp.minimum(good, fine)
                ends.append(1.0 / f)
            okay[:, here] = jnp.minimum(okay[:, here], good)
            p = ends[0] * ends[1] * ends[2]
            e = exclusive(p)
            total = e[0:1, :] * p[0:1, :]
            e = e * start
            s2 = e * ends[2]
            s1 = s2 * ends[1]
            scales = [s1 * ends[0], s1, s2]
        both = [jnp.concatenate([s, s], axis=0) for s in scales]
        parts = []
        for r in range(0, SEG, 2):
            parts.append((wts[r * 8:(r + 2) * 8, here] * both[r // CHUNK]).astype(bf16))
        return start * total, jnp.concatenate(parts, axis=0)

    spots = range(0, COLS, TILE)

    def load(block, k):
        rows = kv_ref[block, 0:BLK, :]
        lk[k, :, 0:128] = rows
        wide = rows.astype(f32)
        turned = pltpu.roll(wide, 64, 1)
        logit = kv_ref[block, BLK:BLK + 8, :].astype(f32)
        lane = lax.broadcasted_iota(jnp.int32, (128, 128), 1)
        for j in range(3):
            column = jnp.broadcast_to(logit[j:j + 1, :], (128, 128)).T
            side = jnp.where(lane < 2, column, jnp.where(lane < 5, 1.0, jnp.where(lane < 64, 0.0, turned[j * 128:(j + 1) * 128, :])))
            lk[k, j * 128:(j + 1) * 128, 128:256] = side.astype(bf16)
        vt[k] = wide.T[64:128, :].astype(bf16)

    def score(half, k, at):
        za[k][:, at:at + TILE] = jnp.dot(lk[k], qt[half, :, at:at + TILE], preferred_element_type=f32)

    def process(half, k, row, slow, after=None):
        starts = [carry[half, :, at:at + TILE] for at in spots]
        for at, start in zip(spots, starts):
            if after is not None:
                score(after, 1 - k, at)
            left, weight = tile(za[k], at, row, slow, start)
            carry[half, :, at:at + TILE] = left
            acc[half, :, at:at + TILE] += jnp.dot(vt[k], weight, preferred_element_type=f32)

    def sweep(slow):
        acc[...] = jnp.zeros_like(acc)
        carry[...] = jnp.ones_like(carry)
        for half, block in ((0, i), (1, n - 1 - i)):
            load(block, 0)
            for at in spots:
                score(half, 0, at)
            process(half, 0, HALF * half, slow)

        def which(s):
            return jnp.where(s < i, 0, 1), jnp.maximum(jnp.where(s < i, i - 1 - s, n - 2 - s), 0)

        half, block = which(0)
        load(block, 0)
        for at in spots:
            score(half, 0, at)

        def pair(t, c):
            for k in range(2):
                half, block = which(2 * t + k)
                after, block = which(2 * t + k + 1)
                load(block, 1 - k)
                process(half, k, None, slow, after)
            return c

        lax.fori_loop(0, (n - 2) // 2, pair, 0)
        process(which(n - 2)[0], 0, None, slow)

    okay[...] = jnp.ones_like(okay)
    sweep(False)

    @pl.when(jnp.min(okay[...]) < 0.5)
    def _():
        sweep(True)

    stacked = jnp.concatenate([acc[0], acc[1]], axis=0).T
    for s in range(2):
        heads = [stacked[h * HALF:(h + 1) * HALF, s * 64:(s + 1) * 64] for h in range(HEADS)]
        out_ref[s * HALF:(s + 1) * HALF, :] = jnp.concatenate(heads, axis=1).astype(bf16)


def attention(n, position, kv, q, offsets):
    vm = pl.BlockSpec(memory_space=pltpu.VMEM)
    sm = pl.BlockSpec(memory_space=pltpu.SMEM)
    return pl.pallas_call(
        functools.partial(attention_kernel, n),
        out_shape=jax.ShapeDtypeStruct((BLK, HEADS * HEAD_DIM), jnp.bfloat16),
        in_specs=[sm, vm, vm, sm],
        out_specs=vm,
        scratch_shapes=[
            pltpu.VMEM((2, 256, COLS), jnp.bfloat16),
            pltpu.VMEM((2, BLK, 256), jnp.bfloat16),
            pltpu.VMEM((2, 64, BLK), jnp.bfloat16),
            pltpu.VMEM((2, 64, COLS), jnp.float32),
            pltpu.VMEM((2, 8, COLS), jnp.float32),
            pltpu.VMEM((8, COLS), jnp.float32),
            pltpu.VMEM((BLK, COLS), jnp.float32),
            pltpu.VMEM((BLK, COLS), jnp.float32),
            pltpu.VMEM((BLK, COLS), jnp.float32),
        ],
        compiler_params=pltpu.CompilerParams(vmem_limit_bytes=40 * 1024 * 1024),
        name="attention",
    )(position, kv, q, offsets)


ROWS = 400
CUT = 192
MESH = pl.DeviceIdType.MESH


def gather_kernel(n, k_ref, v_ref, l_ref, q_ref, kv_ref, qs_ref, send, recv):
    f32, bf16 = jnp.float32, jnp.bfloat16
    me = lax.axis_index("sp")
    z, y, core = lax.div(me, 8), lax.rem(lax.div(me, 2), 4), lax.rem(me, 2)

    def at(a, b, c):
        dz, dy = a * c + b * (1 - c), a * (1 - c) + b * c
        return lax.rem(z + dz, 4) * 8 + lax.rem(y + dy, 4) * 2 + c

    other, mirror = me + 1 - 2 * core, n - 1 - me
    near = [at(1, 0, core), at(3, 0, core)], [at(0, 1, core), at(0, 3, core)]
    far = at(2, 0, core)
    barrier = pltpu.get_barrier_semaphore()
    for peer in near[0] + near[1] + [far, other, mirror]:
        pl.semaphore_signal(barrier, inc=1, device_id={"sp": peer}, device_id_type=MESH)

    spot = lax.broadcasted_iota(jnp.int32, (BLK, BLK), 0)
    source = lax.broadcasted_iota(jnp.int32, (BLK, BLK), 1)
    order = jnp.where(source == (spot % 8) * SEG + spot // 8, 1.0, 0.0).astype(bf16)
    across = (((1,), (1,)), ((), ()))
    both = jnp.concatenate([k_ref[...], v_ref[...]], axis=0)
    kv_ref[me, 0:BLK, :] = lax.dot_general(order, both, across, preferred_element_type=f32).astype(bf16)
    logit = jnp.broadcast_to(l_ref[...].astype(f32), (16, BLK)).astype(bf16)
    logit = lax.dot_general(logit, order, across, preferred_element_type=f32)
    row = lax.broadcasted_iota(jnp.int32, (16, 128), 0)
    tail = jnp.zeros((16, 128), f32)
    for j in range(3):
        tail = jnp.where(row == j, logit[:, j * 128:(j + 1) * 128], tail)
    kv_ref[me, BLK:ROWS, :] = tail.astype(bf16)
    qs_ref[0:HALF, :] = q_ref[0:HALF, :]
    pl.semaphore_wait(barrier, 7)

    begun = []
    parts = (slice(0, ROWS), slice(0, CUT), slice(CUT, ROWS))

    def copy(index, slot, part, peer):
        piece = kv_ref.at[slot, parts[part]]
        return pltpu.make_async_remote_copy(
            src_ref=piece, dst_ref=piece, send_sem=send.at[index], recv_sem=recv.at[index],
            device_id={"sp": peer}, device_id_type=MESH)

    def begin(index, slot, part, peer):
        c = copy(index, slot, part, peer)
        c.start()
        begun.append(c)

    def arrive(index, slot, part):
        copy(index, slot, part, me).wait_recv()

    around = (0, 3, 1, 2)

    def spread(k, a):
        slot = at(a, 0, core)
        for d in range(2):
            begin(4 + 4 * k + d, slot, 0, near[1][d])
        begin(20 + k, slot, 0, other)

    swap = pltpu.make_async_remote_copy(
        src_ref=q_ref.at[HALF:BLK], dst_ref=qs_ref.at[HALF:BLK], send_sem=send.at[36], recv_sem=recv.at[36],
        device_id={"sp": mirror}, device_id_type=MESH)
    for d in range(2):
        begin(d, me, 0, near[0][d])
    begin(2, me, 0, far)
    spread(0, 0)
    swap.start()
    for d, a in ((0, 3), (1, 1)):
        slot = at(a, 0, core)
        arrive(d, slot, 0)
        spread(1 + d, a)
    slot = at(2, 0, core)
    arrive(2, slot, 0)
    spread(3, 2)
    for k, a in enumerate(around):
        for d, b in ((0, 3), (1, 1)):
            slot = at(a, b, core)
            arrive(4 + 4 * k + d, slot, 0)
            begin(6 + 4 * k + d, slot, 1 + d, near[1][d])
            begin(24 + 4 * d + k, slot, 0, other)
    for k, a in enumerate(around):
        slot = at(a, 2, core)
        for d in range(2):
            arrive(6 + 4 * k + d, slot, 1 + d)
        begin(32 + k, slot, 0, other)
    for j, b in enumerate((0, 3, 1, 2)):
        for k, a in enumerate(around):
            arrive(20 + 4 * j + k, at(a, b, 1 - core), 0)
    swap.wait_recv()
    for c in begun:
        c.wait_send()
    swap.wait_send()


def gather(n, k, v, logit, q):
    vm = pl.BlockSpec(memory_space=pltpu.VMEM)
    return pl.pallas_call(
        functools.partial(gather_kernel, n),
        out_shape=(
            jax.ShapeDtypeStruct((n, ROWS, 128), jnp.bfloat16),
            jax.ShapeDtypeStruct((BLK, HEADS * HEAD_DIM), jnp.bfloat16),
        ),
        in_specs=[vm] * 4,
        out_specs=(vm, vm),
        scratch_shapes=[pltpu.SemaphoreType.DMA((37,)), pltpu.SemaphoreType.DMA((37,))],
        compiler_params=pltpu.CompilerParams(collective_id=0, has_side_effects=True, vmem_limit_bytes=24 * 1024 * 1024),
        name="gather",
    )(k, v, logit, q)


WIDTH = 2048
FF_WIDTH = 1024
OWN = 96
CAP = 3
LANES = 128


def moe_kernel(n_sp, n_tp, halves, stream, wo_hbm, gain, ids_ref, group_ref, logit_ref, wg_hbm, wu_hbm, wd_hbm, out_ref,
               wo, wg, wu, wd, heads, mixed, normed, wide, going, coming, leaving, back, rows, hidden, pick, total,
               load, sends, recvs, bulk):
    f32, bf16 = jnp.float32, jnp.bfloat16
    n = n_sp * n_tp
    groups = 4
    slots = n * CAP // groups
    fold = WIDTH // LANES
    unit = CAP * fold
    sp, tp = lax.axis_index("sp"), lax.axis_index("tp")
    me = sp * n_tp + tp
    rem, div = lax.rem, lax.div
    z, y, core = div(sp, 8), rem(div(sp, 2), 4), rem(sp, 2)
    mirror = n_sp - 1 - sp
    xs = [rem(tp + k, 4) for k in range(4)]
    ys = [rem(y + k, 4) * 2 for k in range(4)]
    cs = [core, 1 - core]

    barrier = pltpu.get_barrier_semaphore()

    def greet(dz, c, skip=False):
        base = rem(z + dz, 4) * 8
        for k in range(1 if skip else 0, 32):
            s2 = base + ys[k // 8] + cs[k // 4 % 2]
            pl.semaphore_signal(barrier, inc=1, device_id={"sp": s2, "tp": xs[k % 4]}, device_id_type=MESH)
        return c

    greet(0, 0, True)
    lax.fori_loop(1, 4, greet, 0)
    loads = [pltpu.make_async_copy(wo_hbm, wo, load.at[0]), pltpu.make_async_copy(wg_hbm.at[0], wg, load.at[1]),
             pltpu.make_async_copy(wu_hbm.at[0], wu, load.at[2]), pltpu.make_async_copy(wd_hbm.at[0], wd, load.at[3])]
    for c in loads:
        c.start()

    small = jnp.concatenate([ids_ref[...].astype(f32), logit_ref[...], group_ref[...], jnp.zeros((3, OWN), f32)], axis=0)
    aux = jnp.concatenate([small, jnp.zeros((8, LANES - OWN), f32)], axis=1).T[0:OWN, :]
    lane = lax.broadcasted_iota(jnp.int32, (OWN, n), 1).astype(f32)
    below = lax.broadcasted_iota(jnp.int32, (OWN, OWN), 0) > lax.broadcasted_iota(jnp.int32, (OWN, OWN), 1)
    below = jnp.where(below, 1.0, 0.0).astype(bf16)
    place = lax.broadcasted_iota(jnp.int32, (OWN, slots), 1)
    ahead = jnp.zeros((1, n), f32)
    for k in range(2):
        ids = aux[:, k:k + 1]
        hit = jnp.where(lane == ids, 1.0, 0.0)
        before = jnp.dot(below, hit.astype(bf16), preferred_element_type=f32) + ahead
        rank = jnp.sum(hit * before, axis=1, keepdims=True)
        ahead = ahead + jnp.sum(hit, axis=0, keepdims=True)
        whole = ids.astype(jnp.int32)
        spot = (whole >> 2) * CAP + rank.astype(jnp.int32)
        group = ((whole & 3) + ((whole >> 3) & 3) + (whole >> 5) - (tp + y + z) + 12) & 3
        for g in range(groups):
            pick[k, g] = jnp.where(jnp.logical_and(place == spot, group == g), 1.0, 0.0).astype(bf16)

    pl.semaphore_wait(barrier, n - 1)

    def piece(j, source):
        return pltpu.make_async_remote_copy(
            src_ref=halves.at[j * OWN:(j + 1) * OWN], dst_ref=heads.at[source], send_sem=sends.at[j], recv_sem=recvs.at[source],
            device_id={"sp": sp if j < 2 else mirror, "tp": j}, device_id_type=MESH)

    for j in range(4):
        if j < 2:
            @pl.when(tp == j)
            def _():
                heads[j] = halves[j * OWN:(j + 1) * OWN, :]

            @pl.when(tp != j)
            def _():
                piece(j, tp).start()
        else:
            piece(j, tp).start()
    for p in range(4):
        if p < 2:
            @pl.when(tp != p)
            def _():
                piece(p, p).wait_recv()
        else:
            piece(p, p).wait_recv()

    loads[0].wait()
    every = jnp.concatenate([heads[p] for p in range(4)], axis=1)
    square = jnp.zeros((OWN, 1), f32)
    for at in range(0, WIDTH, 512):
        here = slice(at, at + 512)
        part = stream[:, here].astype(f32) + jnp.dot(every, wo[:, here], preferred_element_type=f32)
        part = part.astype(bf16)
        mixed[:, here] = part
        part = part.astype(f32)
        square = square + jnp.sum(part * part, axis=1, keepdims=True)
    factor = lax.rsqrt(square / WIDTH + norm_eps)
    normed[...] = (mixed[...].astype(f32) * factor * gain[...]).astype(bf16)

    block = slots * fold

    def narrow(target, g):
        for at in range(0, block, 512):
            target[g, at:at + 512, :] = wide[at:at + 512, :].astype(bf16)

    def unfold(origin, g):
        for at in range(0, block, 512):
            wide[at:at + 512, :] = origin[g, at:at + 512, :].astype(f32)
        for c in range(fold):
            rows[:, c * LANES:(c + 1) * LANES] = wide[pl.ds(c, slots, stride=fold), :].astype(bf16)

    def store(at, value):
        for c in range(value.shape[1] // LANES):
            wide[pl.ds(at + c, slots, stride=fold), :] = value[:, c * LANES:(c + 1) * LANES]

    def span_of(d):
        return pl.ds(pl.multiple_of(d * unit, unit), unit)

    def send_group(origin, target, g, k, sign):
        def one(dz, c, skip=False):
            base = rem(z + dz, 4) * 8
            for j in range(1 if skip else 0, 8):
                dy, dc = j // 2, j % 2
                s2 = base + ys[dy] + cs[dc]
                x2 = rem(tp + sign * g - dz - dy + 12, 4)
                pltpu.make_async_remote_copy(
                    src_ref=origin.at[g, span_of(s2)], dst_ref=target.at[g, span_of(sp)], send_sem=bulk.at[k, g], recv_sem=bulk.at[k + 1, g],
                    device_id={"sp": s2, "tp": x2}, device_id_type=MESH).start()
            return c

        if g == 0:
            one(0, 0, True)
            target[g, span_of(sp), :] = origin[g, span_of(sp), :]
        lax.fori_loop(1 if g == 0 else 0, 4, one, 0)

    def rest(origin, target, g, k):
        most = pl.ds(0, (n_sp - 1 if g == 0 else n_sp) * unit)
        return pltpu.make_async_remote_copy(
            src_ref=origin.at[g, most], dst_ref=target.at[g, most], send_sem=bulk.at[k, g], recv_sem=bulk.at[k + 1, g],
            device_id={"sp": mirror, "tp": tp}, device_id_type=MESH)

    for g in range(groups):
        chooser = (pick[0, g] + pick[1, g]).astype(f32).T.astype(bf16)
        for at in range(0, WIDTH, 256):
            store(at // LANES, jnp.dot(chooser, normed[:, at:at + 256], preferred_element_type=f32))
        narrow(going, g)
        send_group(going, coming, g, 0, 1)

    def up(b, c):
        here = pl.ds(pl.multiple_of(b * 512, 512), 512)
        gated = jnp.dot(rows[...], wg[:, here], preferred_element_type=f32)
        raised = jnp.dot(rows[...], wu[:, here], preferred_element_type=f32)
        hidden[:, here] = (gated / (1.0 + jnp.exp(-gated)) * raised).astype(bf16)
        return c

    for g in range(groups):
        rest(going, coming, g, 0).wait_recv()
        unfold(coming, g)
        if g == 0:
            loads[1].wait()
            loads[2].wait()
        lax.fori_loop(0, FF_WIDTH // 512, up, 0)
        if g == 0:
            loads[3].wait()
        for at in range(0, WIDTH, 512):
            store(at // LANES, jnp.dot(hidden[...], wd[:, at:at + 512], preferred_element_type=f32))
        narrow(leaving, g)
        send_group(leaving, back, g, 2, -1)

    high = jnp.maximum(aux[:, 2:3], aux[:, 3:4])
    e0, e1 = jnp.exp(aux[:, 2:3] - high), jnp.exp(aux[:, 3:4] - high)
    scale = 1.0 / (1.0 + jnp.exp(-aux[:, 4:5])) / (e0 + e1)
    for g in range(groups):
        rest(leaving, back, g, 2).wait_recv()
        unfold(back, g)
        for at in range(0, WIDTH, 256):
            here = slice(at, at + 256)
            added = jnp.dot(pick[0, g], rows[:, here], preferred_element_type=f32) * (scale * e0)
            added = added + jnp.dot(pick[1, g], rows[:, here], preferred_element_type=f32) * (scale * e1)
            if g > 0:
                added = added + total[:, here]
            if g < groups - 1:
                total[:, here] = added
            else:
                out_ref[:, here] = (mixed[:, here].astype(f32) + added).astype(bf16)
    for g in range(groups):
        rest(going, coming, g, 0).wait_send()
        rest(leaving, back, g, 2).wait_send()
    for j in range(4):
        if j < 2:
            @pl.when(tp != j)
            def _():
                piece(j, tp).wait_send()
        else:
            piece(j, tp).wait_send()


def moe(n_sp, n_tp, halves, stream, out_weight, gain, ids, group, logits, gate, up, down):
    vm = pl.BlockSpec(memory_space=pltpu.VMEM)
    hbm = pl.BlockSpec(memory_space=pl.ANY)
    groups = 4
    slots = n_sp * n_tp * CAP // groups
    linear = (slots * WIDTH // LANES, LANES)
    grouped = (groups,) + linear
    bf16 = jnp.bfloat16
    dma = pltpu.SemaphoreType.DMA
    return pl.pallas_call(
        functools.partial(moe_kernel, n_sp, n_tp),
        out_shape=jax.ShapeDtypeStruct((OWN, WIDTH), bf16),
        in_specs=[vm, vm, hbm, vm, vm, vm, vm, hbm, hbm, hbm],
        out_specs=vm,
        scratch_shapes=[
            pltpu.VMEM((1024, WIDTH), bf16), pltpu.VMEM((WIDTH, FF_WIDTH), bf16), pltpu.VMEM((WIDTH, FF_WIDTH), bf16), pltpu.VMEM((FF_WIDTH, WIDTH), bf16),
            pltpu.VMEM((4, OWN, 256), bf16), pltpu.VMEM((OWN, WIDTH), bf16), pltpu.VMEM((OWN, WIDTH), bf16),
            pltpu.VMEM(linear, jnp.float32),
            pltpu.VMEM(grouped, bf16), pltpu.VMEM(grouped, bf16), pltpu.VMEM(grouped, bf16), pltpu.VMEM(grouped, bf16),
            pltpu.VMEM((slots, WIDTH), bf16), pltpu.VMEM((slots, FF_WIDTH), bf16), pltpu.VMEM((2, groups, OWN, slots), bf16), pltpu.VMEM((OWN, WIDTH), jnp.float32),
            dma((4,)), dma((4,)), dma((4,)), dma((4, groups)),
        ],
        compiler_params=pltpu.CompilerParams(collective_id=1, has_side_effects=True, vmem_limit_bytes=56 * 1024 * 1024),
        name="experts",
    )(halves, stream, out_weight, gain, ids, group, logits, gate, up, down)


def on_device(
    queries,
    key_rows,
    value_rows,
    key_logit,
    head_offset,
    stream,
    out_weight,
    norm_gain,
    expert_ids,
    group_logit,
    expert_logits,
    gate_weight,
    up_weight,
    down_weight,
):
    n_sp, n_tp = lax.axis_size("sp"), lax.axis_size("tp")
    position = lax.axis_index("sp").astype(jnp.int32).reshape(1)
    kv, chosen = gather(n_sp, key_rows.T, value_rows.T, key_logit.T, queries)
    halves = attention(n_sp, position, kv, chosen, head_offset)
    return moe(n_sp, n_tp, halves, stream, out_weight, norm_gain[None], expert_ids.T, group_logit[None], expert_logits.T, gate_weight, up_weight, down_weight)


def solution(mesh):
    placed = (
        P("sp", "tp"),
        P("sp", "tp"),
        P("sp", "tp"),
        P("sp", "tp"),
        P("tp"),
        P(("sp", "tp"), None),
        P(),
        P(),
        P(("sp", "tp"), None),
        P(("sp", "tp")),
        P(("sp", "tp"), None),
        P(("sp", "tp"), None, None),
        P(("sp", "tp"), None, None),
        P(("sp", "tp"), None, None),
    )
    return jax.shard_map(
        on_device, mesh=mesh, in_specs=placed, out_specs=P(("sp", "tp"), None), check_vma=False
    )
```

```python
import functools

import jax
import jax.numpy as jnp
from jax import lax
from jax.experimental import pallas as pl
from jax.experimental.pallas import tpu as pltpu
from jax.sharding import PartitionSpec as P

HEAD_DIM = 64
norm_eps = 1e-06
HEADS = 4
BLK = 384
HALF = 192
SEG = 48
CHUNK = 16
COLS = 768
TILE = 768
LOG2E = 1.4426950408889634


def split3(x):
    hi = x.astype(jnp.bfloat16).astype(jnp.float32)
    rest = x - hi
    mid = rest.astype(jnp.bfloat16).astype(jnp.float32)
    lo = (rest - mid).astype(jnp.bfloat16).astype(jnp.float32)
    return hi, mid, lo


def attention_kernel(n, pos_ref, kv_ref, off_ref, out_ref, qt, lk, vt, acc, carry, okay, wts, z0, z1):
    i = pos_ref[0]
    za = (z0, z1)
    f32, bf16 = jnp.float32, jnp.bfloat16
    for s in range(2):
        qs = jnp.concatenate([kv_ref[n + j, s * HALF:(s + 1) * HALF, :].astype(f32) for j in range(2)], axis=1) * (LOG2E * HEAD_DIM ** -0.5)
        rows = jnp.concatenate([qs[:, h * 64:(h + 1) * 64] for h in range(HEADS)], axis=0)
        high = rows.astype(bf16).astype(f32)
        low = rows - high
        zero = jnp.zeros_like(rows)
        top = jnp.concatenate([high, zero], axis=1).T
        bottom = jnp.concatenate([zero, low], axis=1).T
        lane = lax.broadcasted_iota(jnp.int32, (8, COLS), 1)
        off = jnp.zeros((8, COLS), f32)
        for h in range(HEADS):
            inside = jnp.logical_and(lane >= h * HALF, lane < (h + 1) * HALF)
            off = jnp.where(inside, off_ref[h] * LOG2E, off)
        hi, mid, lo = split3(off)
        row = lax.broadcasted_iota(jnp.int32, (8, COLS), 0)
        c_hi = 1.4453125
        extra = jnp.where(row == 0, c_hi, jnp.where(row == 1, LOG2E - c_hi, jnp.where(row == 2, hi, jnp.where(row == 3, mid, jnp.where(row == 4, lo, 0.0)))))
        bottom = jnp.concatenate([extra, bottom[8:, :]], axis=0)
        qt[s, 0:128, :] = top.astype(bf16)
        qt[s, 128:256, :] = bottom.astype(bf16)

    sub = lax.broadcasted_iota(jnp.int32, (8, TILE), 0)

    def exclusive(p):
        e = jnp.where(sub == 7, 1.0, pltpu.roll(p, 7, 0))
        e = e * jnp.where(sub == 7, 1.0, pltpu.roll(e, 7, 0))
        e = e * jnp.where(sub >= 6, 1.0, pltpu.roll(e, 6, 0))
        e = e * jnp.where(sub >= 4, 1.0, pltpu.roll(e, 4, 0))
        return e

    def tile(zs, at, row, slow, start):
        here = slice(at, at + TILE)
        if row is not None:
            lane = lax.broadcasted_iota(jnp.int32, (8, TILE), 1)
            limit = (lane + at) % HALF + row - sub * SEG
        if slow:
            p = jnp.ones((8, TILE), f32)
            for r in reversed(range(SEG)):
                beta = 1.0 / (1.0 + jnp.exp2(-zs[r * 8:(r + 1) * 8, here]))
                if row is not None:
                    beta = jnp.where(r < limit, beta, 0.0)
                w = p * beta
                p = p - w
                wts[r * 8:(r + 1) * 8, here] = w
            e = exclusive(p)
            total = e[0:1, :] * p[0:1, :]
            e = e * start
            scales = [e] * (SEG // CHUNK)
        else:
            ends, good = [], None
            for ch in range(SEG // CHUNK):
                f = jnp.ones((8, TILE), f32)
                for r in range(ch * CHUNK, (ch + 1) * CHUNK):
                    x = jnp.exp2(zs[r * 8:(r + 1) * 8, here])
                    if row is not None:
                        x = jnp.where(r < limit, x, 0.0)
                    w = x * f
                    f = f + w
                    wts[r * 8:(r + 1) * 8, here] = w
                fine = jnp.where(f < 1e36, 1.0, 0.0)
                good = fine if good is None else jnp.minimum(good, fine)
                ends.append(1.0 / f)
            okay[:, here] = jnp.minimum(okay[:, here], good)
            p = ends[0] * ends[1] * ends[2]
            e = exclusive(p)
            total = e[0:1, :] * p[0:1, :]
            e = e * start
            s2 = e * ends[2]
            s1 = s2 * ends[1]
            scales = [s1 * ends[0], s1, s2]
        both = [jnp.concatenate([s, s], axis=0) for s in scales]
        parts = []
        for r in range(0, SEG, 2):
            parts.append((wts[r * 8:(r + 2) * 8, here] * both[r // CHUNK]).astype(bf16))
        return start * total, jnp.concatenate(parts, axis=0)

    spots = range(0, COLS, TILE)

    def load(block, k):
        rows = kv_ref[block, 0:BLK, :]
        lk[k, :, 0:128] = rows
        wide = rows.astype(f32)
        turned = pltpu.roll(wide, 64, 1)
        logit = kv_ref[block, BLK:BLK + 8, :].astype(f32)
        lane = lax.broadcasted_iota(jnp.int32, (128, 128), 1)
        for j in range(3):
            column = jnp.broadcast_to(logit[j:j + 1, :], (128, 128)).T
            side = jnp.where(lane < 2, column, jnp.where(lane < 5, 1.0, jnp.where(lane < 64, 0.0, turned[j * 128:(j + 1) * 128, :])))
            lk[k, j * 128:(j + 1) * 128, 128:256] = side.astype(bf16)
        vt[k] = wide.T[64:128, :].astype(bf16)

    def score(half, k, at):
        za[k][:, at:at + TILE] = jnp.dot(lk[k], qt[half, :, at:at + TILE], preferred_element_type=f32)

    def process(half, k, row, slow, after=None):
        starts = [carry[half, :, at:at + TILE] for at in spots]
        for at, start in zip(spots, starts):
            if after is not None:
                score(after, 1 - k, at)
            left, weight = tile(za[k], at, row, slow, start)
            carry[half, :, at:at + TILE] = left
            acc[half, :, at:at + TILE] += jnp.dot(vt[k], weight, preferred_element_type=f32)

    def sweep(slow):
        acc[...] = jnp.zeros_like(acc)
        carry[...] = jnp.ones_like(carry)
        for half, block in ((0, i), (1, n - 1 - i)):
            load(block, 0)
            for at in spots:
                score(half, 0, at)
            process(half, 0, HALF * half, slow)

        def which(s):
            return jnp.where(s < i, 0, 1), jnp.maximum(jnp.where(s < i, i - 1 - s, n - 2 - s), 0)

        half, block = which(0)
        load(block, 0)
        for at in spots:
            score(half, 0, at)

        def pair(t, c):
            for k in range(2):
                half, block = which(2 * t + k)
                after, block = which(2 * t + k + 1)
                load(block, 1 - k)
                process(half, k, None, slow, after)
            return c

        lax.fori_loop(0, (n - 2) // 2, pair, 0)
        process(which(n - 2)[0], 0, None, slow)

    okay[...] = jnp.ones_like(okay)
    sweep(False)

    @pl.when(jnp.min(okay[...]) < 0.5)
    def _():
        sweep(True)

    stacked = jnp.concatenate([acc[0], acc[1]], axis=0).T
    for s in range(2):
        heads = [stacked[h * HALF:(h + 1) * HALF, s * 64:(s + 1) * 64] for h in range(HEADS)]
        out_ref[s * HALF:(s + 1) * HALF, :] = jnp.concatenate(heads, axis=1).astype(bf16)


def attention(n, position, kv, offsets):
    vm = pl.BlockSpec(memory_space=pltpu.VMEM)
    sm = pl.BlockSpec(memory_space=pltpu.SMEM)
    return pl.pallas_call(
        functools.partial(attention_kernel, n),
        out_shape=jax.ShapeDtypeStruct((BLK, HEADS * HEAD_DIM), jnp.bfloat16),
        in_specs=[sm, vm, sm],
        out_specs=vm,
        scratch_shapes=[
            pltpu.VMEM((2, 256, COLS), jnp.bfloat16),
            pltpu.VMEM((2, BLK, 256), jnp.bfloat16),
            pltpu.VMEM((2, 64, BLK), jnp.bfloat16),
            pltpu.VMEM((2, 64, COLS), jnp.float32),
            pltpu.VMEM((2, 8, COLS), jnp.float32),
            pltpu.VMEM((8, COLS), jnp.float32),
            pltpu.VMEM((BLK, COLS), jnp.float32),
            pltpu.VMEM((BLK, COLS), jnp.float32),
            pltpu.VMEM((BLK, COLS), jnp.float32),
        ],
        compiler_params=pltpu.CompilerParams(vmem_limit_bytes=20 * 1024 * 1024),
        name="attention",
    )(position, kv, offsets)


ROWS = 400
CUT = 192
MESH = pl.DeviceIdType.MESH


def gather_kernel(n, k_ref, v_ref, l_ref, q_ref, kv_ref, send, recv):
    f32, bf16 = jnp.float32, jnp.bfloat16
    me = lax.axis_index("sp")
    z, y, core = lax.div(me, 8), lax.rem(lax.div(me, 2), 4), lax.rem(me, 2)

    def at(a, b, c):
        dz, dy = a * c + b * (1 - c), a * (1 - c) + b * c
        return lax.rem(z + dz, 4) * 8 + lax.rem(y + dy, 4) * 2 + c

    other, mirror = me + 1 - 2 * core, n - 1 - me
    near = [at(1, 0, core), at(3, 0, core)], [at(0, 1, core), at(0, 3, core)]
    far = at(2, 0, core)
    barrier = pltpu.get_barrier_semaphore()
    for peer in near[0] + near[1] + [far, other, mirror]:
        pl.semaphore_signal(barrier, inc=1, device_id={"sp": peer}, device_id_type=MESH)

    spot = lax.broadcasted_iota(jnp.int32, (BLK, BLK), 0)
    source = lax.broadcasted_iota(jnp.int32, (BLK, BLK), 1)
    order = jnp.where(source == (spot % 8) * SEG + spot // 8, 1.0, 0.0).astype(bf16)
    across = (((1,), (1,)), ((), ()))
    both = jnp.concatenate([k_ref[...], v_ref[...]], axis=0)
    kv_ref[me, 0:BLK, :] = lax.dot_general(order, both, across, preferred_element_type=f32).astype(bf16)
    logit = jnp.broadcast_to(l_ref[...].astype(f32), (16, BLK)).astype(bf16)
    logit = lax.dot_general(logit, order, across, preferred_element_type=f32)
    row = lax.broadcasted_iota(jnp.int32, (16, 128), 0)
    tail = jnp.zeros((16, 128), f32)
    for j in range(3):
        tail = jnp.where(row == j, logit[:, j * 128:(j + 1) * 128], tail)
    kv_ref[me, BLK:ROWS, :] = tail.astype(bf16)
    for j in range(2):
        kv_ref[n + j, 0:HALF, :] = q_ref[0:HALF, j * 128:(j + 1) * 128]
    pl.semaphore_wait(barrier, 7)

    begun = []
    parts = (slice(0, ROWS), slice(0, CUT), slice(CUT, ROWS))

    def copy(index, slot, part, peer):
        piece = kv_ref.at[slot, parts[part]]
        return pltpu.make_async_remote_copy(
            src_ref=piece, dst_ref=piece, send_sem=send.at[index], recv_sem=recv.at[index],
            device_id={"sp": peer}, device_id_type=MESH)

    def begin(index, slot, part, peer):
        c = copy(index, slot, part, peer)
        c.start()
        begun.append(c)

    def arrive(index, slot, part):
        copy(index, slot, part, me).wait_recv()

    around = (0, 3, 1, 2)

    def spread(k, a):
        slot = at(a, 0, core)
        for d in range(2):
            begin(4 + 4 * k + d, slot, 0, near[1][d])
        begin(20 + k, slot, 0, other)

    swaps = [pltpu.make_async_remote_copy(
        src_ref=q_ref.at[HALF:BLK, j * 128:(j + 1) * 128], dst_ref=kv_ref.at[n + j, HALF:BLK], send_sem=send.at[36 + j], recv_sem=recv.at[36 + j],
        device_id={"sp": mirror}, device_id_type=MESH) for j in range(2)]
    for d in range(2):
        begin(d, me, 0, near[0][d])
    begin(2, me, 0, far)
    spread(0, 0)
    for c in swaps:
        c.start()
    for d, a in ((0, 3), (1, 1)):
        slot = at(a, 0, core)
        arrive(d, slot, 0)
        spread(1 + d, a)
    slot = at(2, 0, core)
    arrive(2, slot, 0)
    spread(3, 2)
    for k, a in enumerate(around):
        for d, b in ((0, 3), (1, 1)):
            slot = at(a, b, core)
            arrive(4 + 4 * k + d, slot, 0)
            begin(6 + 4 * k + d, slot, 1 + d, near[1][d])
            begin(24 + 4 * d + k, slot, 0, other)
    for k, a in enumerate(around):
        slot = at(a, 2, core)
        for d in range(2):
            arrive(6 + 4 * k + d, slot, 1 + d)
        begin(32 + k, slot, 0, other)
    for j, b in enumerate((0, 3, 1, 2)):
        for k, a in enumerate(around):
            arrive(20 + 4 * j + k, at(a, b, 1 - core), 0)
    for c in begun:
        c.wait_send()
    for c in swaps:
        c.wait()


def gather(n, k, v, logit, q):
    vm = pl.BlockSpec(memory_space=pltpu.VMEM)
    return pl.pallas_call(
        functools.partial(gather_kernel, n),
        out_shape=jax.ShapeDtypeStruct((n + 2, ROWS, 128), jnp.bfloat16),
        in_specs=[vm] * 4,
        out_specs=vm,
        scratch_shapes=[pltpu.SemaphoreType.DMA((38,)), pltpu.SemaphoreType.DMA((38,))],
        compiler_params=pltpu.CompilerParams(collective_id=0, has_side_effects=True, vmem_limit_bytes=16 * 1024 * 1024),
        name="gather",
    )(k, v, logit, q)


WIDTH = 2048
FF_WIDTH = 1024
OWN = 96
CAP = 3
LANES = 128


def moe_kernel(n_sp, n_tp, halves, stream, wo_hbm, gain, ids_ref, group_ref, logit_ref, wg_hbm, wu_hbm, wd_hbm, out_ref,
               wo, wg, wu, wd, heads, mixed, normed, wide, going, coming, leaving, back, rows, hidden, pick, total,
               load, sends, recvs, bulk):
    f32, bf16 = jnp.float32, jnp.bfloat16
    n = n_sp * n_tp
    groups = 4
    slots = n * CAP // groups
    fold = WIDTH // LANES
    unit = CAP * fold
    sp, tp = lax.axis_index("sp"), lax.axis_index("tp")
    me = sp * n_tp + tp
    rem, div = lax.rem, lax.div
    z, y, core = div(sp, 8), rem(div(sp, 2), 4), rem(sp, 2)
    mirror = n_sp - 1 - sp
    xs = [rem(tp + k, 4) for k in range(4)]
    ys = [rem(y + k, 4) * 2 for k in range(4)]
    cs = [core, 1 - core]

    barrier = pltpu.get_barrier_semaphore()

    def greet(dz, c, skip=False):
        base = rem(z + dz, 4) * 8
        for k in range(1 if skip else 0, 32):
            s2 = base + ys[k // 8] + cs[k // 4 % 2]
            pl.semaphore_signal(barrier, inc=1, device_id={"sp": s2, "tp": xs[k % 4]}, device_id_type=MESH)
        return c

    greet(0, 0, True)
    lax.fori_loop(1, 4, greet, 0)
    loads = [pltpu.make_async_copy(wo_hbm, wo, load.at[0]), pltpu.make_async_copy(wg_hbm.at[0], wg, load.at[1]),
             pltpu.make_async_copy(wu_hbm.at[0], wu, load.at[2]), pltpu.make_async_copy(wd_hbm.at[0], wd, load.at[3])]
    for c in loads:
        c.start()

    small = jnp.concatenate([ids_ref[...].astype(f32), logit_ref[...], group_ref[...], jnp.zeros((3, OWN), f32)], axis=0)
    aux = jnp.concatenate([small, jnp.zeros((8, LANES - OWN), f32)], axis=1).T[0:OWN, :]
    lane = lax.broadcasted_iota(jnp.int32, (OWN, n), 1).astype(f32)
    below = lax.broadcasted_iota(jnp.int32, (OWN, OWN), 0) > lax.broadcasted_iota(jnp.int32, (OWN, OWN), 1)
    below = jnp.where(below, 1.0, 0.0).astype(bf16)
    place = lax.broadcasted_iota(jnp.int32, (OWN, slots), 1)
    ahead = jnp.zeros((1, n), f32)
    for k in range(2):
        ids = aux[:, k:k + 1]
        hit = jnp.where(lane == ids, 1.0, 0.0)
        before = jnp.dot(below, hit.astype(bf16), preferred_element_type=f32) + ahead
        rank = jnp.sum(hit * before, axis=1, keepdims=True)
        ahead = ahead + jnp.sum(hit, axis=0, keepdims=True)
        whole = ids.astype(jnp.int32)
        spot = (whole >> 2) * CAP + rank.astype(jnp.int32)
        group = ((whole & 3) + ((whole >> 3) & 3) + (whole >> 5) - (tp + y + z) + 12) & 3
        for g in range(groups):
            pick[k, g] = jnp.where(jnp.logical_and(place == spot, group == g), 1.0, 0.0).astype(bf16)

    pl.semaphore_wait(barrier, n - 1)

    def piece(j, source):
        return pltpu.make_async_remote_copy(
            src_ref=halves.at[j * OWN:(j + 1) * OWN], dst_ref=heads.at[source], send_sem=sends.at[j], recv_sem=recvs.at[source],
            device_id={"sp": sp if j < 2 else mirror, "tp": j}, device_id_type=MESH)

    for j in range(4):
        if j < 2:
            @pl.when(tp == j)
            def _():
                heads[j] = halves[j * OWN:(j + 1) * OWN, :]

            @pl.when(tp != j)
            def _():
                piece(j, tp).start()
        else:
            piece(j, tp).start()
    for p in range(4):
        if p < 2:
            @pl.when(tp != p)
            def _():
                piece(p, p).wait_recv()
        else:
            piece(p, p).wait_recv()

    loads[0].wait()
    every = jnp.concatenate([heads[p] for p in range(4)], axis=1)
    square = jnp.zeros((OWN, 1), f32)
    for at in range(0, WIDTH, 512):
        here = slice(at, at + 512)
        part = stream[:, here].astype(f32) + jnp.dot(every, wo[:, here], preferred_element_type=f32)
        part = part.astype(bf16)
        mixed[:, here] = part
        part = part.astype(f32)
        square = square + jnp.sum(part * part, axis=1, keepdims=True)
    factor = lax.rsqrt(square / WIDTH + norm_eps)
    normed[...] = (mixed[...].astype(f32) * factor * gain[...]).astype(bf16)

    block = slots * fold

    def narrow(target, g):
        for at in range(0, block, 512):
            target[g, at:at + 512, :] = wide[at:at + 512, :].astype(bf16)

    def unfold(origin, g):
        for at in range(0, block, 512):
            wide[at:at + 512, :] = origin[g, at:at + 512, :].astype(f32)
        for c in range(fold):
            rows[:, c * LANES:(c + 1) * LANES] = wide[pl.ds(c, slots, stride=fold), :].astype(bf16)

    def store(at, value):
        for c in range(value.shape[1] // LANES):
            wide[pl.ds(at + c, slots, stride=fold), :] = value[:, c * LANES:(c + 1) * LANES]

    def span_of(d):
        return pl.ds(pl.multiple_of(d * unit, unit), unit)

    def send_group(origin, target, g, k, sign):
        def one(dz, c, skip=False):
            base = rem(z + dz, 4) * 8
            for j in range(1 if skip else 0, 8):
                dy, dc = j // 2, j % 2
                s2 = base + ys[dy] + cs[dc]
                x2 = rem(tp + sign * g - dz - dy + 12, 4)
                pltpu.make_async_remote_copy(
                    src_ref=origin.at[g, span_of(s2)], dst_ref=target.at[g, span_of(sp)], send_sem=bulk.at[k, g], recv_sem=bulk.at[k + 1, g],
                    device_id={"sp": s2, "tp": x2}, device_id_type=MESH).start()
            return c

        if g == 0:
            one(0, 0, True)
            target[g, span_of(sp), :] = origin[g, span_of(sp), :]
        lax.fori_loop(1 if g == 0 else 0, 4, one, 0)

    def rest(origin, target, g, k):
        most = pl.ds(0, (n_sp - 1 if g == 0 else n_sp) * unit)
        return pltpu.make_async_remote_copy(
            src_ref=origin.at[g, most], dst_ref=target.at[g, most], send_sem=bulk.at[k, g], recv_sem=bulk.at[k + 1, g],
            device_id={"sp": mirror, "tp": tp}, device_id_type=MESH)

    for g in range(groups):
        chooser = (pick[0, g] + pick[1, g]).astype(f32).T.astype(bf16)
        for at in range(0, WIDTH, 256):
            store(at // LANES, jnp.dot(chooser, normed[:, at:at + 256], preferred_element_type=f32))
        narrow(going, g)
        send_group(going, coming, g, 0, 1)

    def up(b, c):
        here = slice(0, FF_WIDTH)
        gated = jnp.dot(rows[...], wg[:, here], preferred_element_type=f32)
        raised = jnp.dot(rows[...], wu[:, here], preferred_element_type=f32)
        hidden[:, here] = (gated / (1.0 + jnp.exp(-gated)) * raised).astype(bf16)
        return c

    for g in range(groups):
        rest(going, coming, g, 0).wait_recv()
        unfold(coming, g)
        if g == 0:
            loads[1].wait()
            loads[2].wait()
        up(0, 0)
        if g == 0:
            loads[3].wait()
        for at in range(0, WIDTH, 512):
            store(at // LANES, jnp.dot(hidden[...], wd[:, at:at + 512], preferred_element_type=f32))
        narrow(leaving, g)
        send_group(leaving, back, g, 2, -1)

    high = jnp.maximum(aux[:, 2:3], aux[:, 3:4])
    e0, e1 = jnp.exp(aux[:, 2:3] - high), jnp.exp(aux[:, 3:4] - high)
    scale = 1.0 / (1.0 + jnp.exp(-aux[:, 4:5])) / (e0 + e1)
    for g in range(groups):
        rest(leaving, back, g, 2).wait_recv()
        unfold(back, g)
        for at in range(0, WIDTH, 256):
            here = slice(at, at + 256)
            added = jnp.dot(pick[0, g], rows[:, here], preferred_element_type=f32) * (scale * e0)
            added = added + jnp.dot(pick[1, g], rows[:, here], preferred_element_type=f32) * (scale * e1)
            if g > 0:
                added = added + total[:, here]
            if g < groups - 1:
                total[:, here] = added
            else:
                out_ref[:, here] = (mixed[:, here].astype(f32) + added).astype(bf16)
    for g in range(groups):
        rest(going, coming, g, 0).wait_send()
        rest(leaving, back, g, 2).wait_send()
    for j in range(4):
        if j < 2:
            @pl.when(tp != j)
            def _():
                piece(j, tp).wait_send()
        else:
            piece(j, tp).wait_send()


def moe(n_sp, n_tp, halves, stream, out_weight, gain, ids, group, logits, gate, up, down):
    vm = pl.BlockSpec(memory_space=pltpu.VMEM)
    hbm = pl.BlockSpec(memory_space=pl.ANY)
    groups = 4
    slots = n_sp * n_tp * CAP // groups
    linear = (slots * WIDTH // LANES, LANES)
    grouped = (groups,) + linear
    bf16 = jnp.bfloat16
    dma = pltpu.SemaphoreType.DMA
    return pl.pallas_call(
        functools.partial(moe_kernel, n_sp, n_tp),
        out_shape=jax.ShapeDtypeStruct((OWN, WIDTH), bf16),
        in_specs=[vm, vm, hbm, vm, vm, vm, vm, hbm, hbm, hbm],
        out_specs=vm,
        scratch_shapes=[
            pltpu.VMEM((1024, WIDTH), bf16), pltpu.VMEM((WIDTH, FF_WIDTH), bf16), pltpu.VMEM((WIDTH, FF_WIDTH), bf16), pltpu.VMEM((FF_WIDTH, WIDTH), bf16),
            pltpu.VMEM((4, OWN, 256), bf16), pltpu.VMEM((OWN, WIDTH), bf16), pltpu.VMEM((OWN, WIDTH), bf16),
            pltpu.VMEM(linear, jnp.float32),
            pltpu.VMEM(grouped, bf16), pltpu.VMEM(grouped, bf16), pltpu.VMEM(grouped, bf16), pltpu.VMEM(grouped, bf16),
            pltpu.VMEM((slots, WIDTH), bf16), pltpu.VMEM((slots, FF_WIDTH), bf16), pltpu.VMEM((2, groups, OWN, slots), bf16), pltpu.VMEM((OWN, WIDTH), jnp.float32),
            dma((4,)), dma((4,)), dma((4,)), dma((4, groups)),
        ],
        compiler_params=pltpu.CompilerParams(collective_id=1, has_side_effects=True, vmem_limit_bytes=56 * 1024 * 1024),
        name="experts",
    )(halves, stream, out_weight, gain, ids, group, logits, gate, up, down)


def on_device(
    queries,
    key_rows,
    value_rows,
    key_logit,
    head_offset,
    stream,
    out_weight,
    norm_gain,
    expert_ids,
    group_logit,
    expert_logits,
    gate_weight,
    up_weight,
    down_weight,
):
    n_sp, n_tp = lax.axis_size("sp"), lax.axis_size("tp")
    position = lax.axis_index("sp").astype(jnp.int32).reshape(1)
    kv = gather(n_sp, key_rows.T, value_rows.T, key_logit.T, queries)
    halves = attention(n_sp, position, kv, head_offset)
    return moe(n_sp, n_tp, halves, stream, out_weight, norm_gain[None], expert_ids.T, group_logit[None], expert_logits.T, gate_weight, up_weight, down_weight)


def solution(mesh):
    placed = (
        P("sp", "tp"),
        P("sp", "tp"),
        P("sp", "tp"),
        P("sp", "tp"),
        P("tp"),
        P(("sp", "tp"), None),
        P(),
        P(),
        P(("sp", "tp"), None),
        P(("sp", "tp")),
        P(("sp", "tp"), None),
        P(("sp", "tp"), None, None),
        P(("sp", "tp"), None, None),
        P(("sp", "tp"), None, None),
    )
    return jax.shard_map(
        on_device, mesh=mesh, in_specs=placed, out_specs=P(("sp", "tp"), None), check_vma=False
    )
```
